256 devices in a mesh: sp: 64 (over z, y, core), tp: 4 (over x).
Axes of the slice: x: 4, y: 4, z: 8, core: 2. Of those that a mesh axis runs over, the one named last changes fastest.
Arguments:
- tokens_in: bfloat16 [16384, 2048], P('sp'), may hold values from -3 to 3
- queries: bfloat16 [16384, 1024], P('sp', 'tp'), may hold values from -6 to 6
- keys: bfloat16 [16384, 256], P('sp', 'tp'), may hold values from -6 to 6
- values: bfloat16 [16384, 256], P('sp', 'tp'), may hold values from -12 to 12
- doc_ids: int32 [16384], P('sp'), may hold values from 0 to 15, never falling along the last dimension, each value on 1 to 8448 neighbouring positions
- query_gain: float32 [64], replicated, may hold values from 2.5 to 6
- key_norm_scale: float32 [64], replicated, may hold values from 2.5 to 6
- out_weight: bfloat16 [1024, 2048], P('tp'), may hold values from -0.1875 to 0.1875
- norm_gain: float32 [2048], replicated, may hold values from 0.1 to 1.9
- gate_weight: bfloat16 [2048, 5632], P('sp', 'tp'), may hold values from -0.125 to 0.125
- up_weight: bfloat16 [2048, 5632], P('sp', 'tp'), may hold values from -0.125 to 0.125
- down_weight: bfloat16 [5632, 2048], P('tp', 'sp'), may hold values from -0.078125 to 0.078125
Outputs:
- layer_out: bfloat16 [16384, 2048], P('sp')
The draws below stay inside these ranges and needn't reach their ends.
Inputs may be any that keep to these rules, and one draw needn't show every extreme that they name: `doc_ids`: document numbers never fall along the sequence; every document has 1 to 8448 positions and one has exactly 8448.
All inputs are finite; a program needn't handle non-finite values.
Results may differ from the reference program's by a relative error of at most 0.014.
The reference program's roundings to bfloat16 on the way (of `weights`, `attended`, `normed` and `hidden`) count: a program that leaves them out, or rounds other values in their place, can miss the bound.
Values may be sent and summed in bfloat16 or wider, within the bound.
A program may use at most 128 MiB of HBM per device.

```python
import math
import jax
import jax.numpy as jnp
import numpy as np
from jax import lax

D = 2048
QUERY_HEADS = 16
KEY_VALUE_HEADS = 4
HEAD_SIZE = 64
FF = 5632
GRID = 64
PACKED_TOKENS = 16384
DOCS = 16
DOC_MOST = 8448
N_TP = 4


def repeated_keys(key):
    sampled_values = jax.random.normal(jax.random.fold_in(key, 11), (PACKED_TOKENS, KEY_VALUE_HEADS * HEAD_SIZE), jnp.float32)
    return jnp.clip(sampled_values, -6.0, 6.0)


def draw_keys(key, part):
    return repeated_keys(key).astype(jnp.bfloat16)


def draw_queries(key, part):
    fresh = jnp.clip(jax.random.normal(jax.random.fold_in(key, 12), (PACKED_TOKENS, QUERY_HEADS * HEAD_SIZE), jnp.float32), -6.0, 6.0)
    return fresh.astype(jnp.bfloat16)


def draw_query_gain(key, part):
    spread = jax.random.uniform(jax.random.fold_in(key, 21), (HEAD_SIZE,), jnp.float32)
    return 2.5 + spread


def draw_key_norm_scale(key, part):
    spread = jax.random.uniform(jax.random.fold_in(key, 22), (HEAD_SIZE,), jnp.float32)
    return 2.5 + spread


def shard_levels(own_key, extent, shards, least, largest):
    def one(dim, parts):
        heights = jax.random.uniform(jax.random.fold_in(jax.random.fold_in(own_key, 6), dim), (parts,), jnp.float32, least / len(shards), largest / len(shards))
        return jnp.repeat(jnp.exp(heights), extent[dim] // parts).reshape((-1,) + (1,) * (len(extent) - dim - 1))

    level = one(*shards[0])
    for cut in shards[1:]:
        level = level * one(*cut)
    return level


def split_up(amount, total, bound, skew):
    loads = [(1 << 20) // math.isqrt(rank ** skew) + 1 for rank in range(2, amount + 1)]
    surplus, counts = total - bound - (amount - 1), [1] * (amount - 1)
    while surplus > 0:
        movable = [i for i in range(amount - 1) if counts[i] < bound]
        mass, remaining = sum([loads[i] for i in movable]), surplus
        for i in movable:
            more = min(bound - counts[i], max(1, remaining * loads[i] // mass), surplus)
            counts[i] = counts[i] + more
            surplus = surplus - more
    return np.array([bound] + counts)


def ragged_sizes(stream_key, amount, total, limit, lean):
    if amount == 2:
        one = jax.random.randint(stream_key, (), max(1, total - limit), min(limit, total - 1) + 1)
        return jnp.stack([one, total - one])
    lengths = jnp.asarray(split_up(amount, total, limit, lean), jnp.int32)
    couples = (amount - 1) // 2
    giver, receiver = lengths[1:1 + 2 * couples:2], lengths[2:2 + 2 * couples:2]
    margin = jnp.minimum(giver - 1, limit - receiver)
    moved = jax.random.randint(jax.random.fold_in(stream_key, 1), (couples,), 0, 1 << 20) % (margin + 1)
    lengths = lengths.at[1:1 + 2 * couples:2].set(giver - moved).at[2:2 + 2 * couples:2].set(receiver + moved)
    return lengths[jax.random.permutation(jax.random.fold_in(stream_key, 2), amount)]


def scatter_about(own_key, dims, width, bound, shards=(), kind=jnp.bfloat16):
    level = shard_levels(own_key, dims, shards, -0.22, 0.18) if shards else 1.0
    drawn = jax.random.normal(own_key, dims, jnp.float32) * width * level
    return jnp.minimum(jnp.maximum(drawn, -bound), bound).astype(kind)


def setup_inputs(seed: int = 0) -> dict:
    key_list = jax.random.split(jax.random.key(seed), 13)
    return {
        "tokens_in": scatter_about(key_list[0], (PACKED_TOKENS, D), 0.5, 3.0, ((0, 64),)),
        "queries": draw_queries(jax.random.fold_in(key_list[12], 71), 0),
        "keys": draw_keys(jax.random.fold_in(key_list[12], 71), 0),
        "values": scatter_about(key_list[3], (PACKED_TOKENS, KEY_VALUE_HEADS * HEAD_SIZE), 2.0, 12.0, ((0, 64), (1, 4))),
        "doc_ids": jnp.searchsorted(jnp.cumsum(ragged_sizes(key_list[4], DOCS, PACKED_TOKENS, DOC_MOST, 1)), jnp.arange(PACKED_TOKENS), side="right").astype(jnp.int32),
        "query_gain": draw_query_gain(jax.random.fold_in(key_list[12], 71), 0),
        "key_norm_scale": draw_key_norm_scale(jax.random.fold_in(key_list[12], 71), 0),
        "out_weight": scatter_about(key_list[7], (QUERY_HEADS * HEAD_SIZE, D), (QUERY_HEADS * HEAD_SIZE) ** -0.5, 0.1875, ((0, 4),)),
        "norm_gain": jnp.clip(1.0 + 0.18 * jax.random.normal(key_list[8], (D,), jnp.float32), 0.1, 1.9),
        "gate_weight": scatter_about(key_list[9], (D, FF), D ** -0.5, 0.125, ((0, 64), (1, 4))),
        "up_weight": scatter_about(key_list[10], (D, FF), D ** -0.5, 0.125, ((0, 64), (1, 4))),
        "down_weight": scatter_about(key_list[11], (FF, D), FF ** -0.5, 0.078125, ((0, 4), (1, 64))),
    }


EPS = 1e-06
THETA = 10000.0
NEG = -1e+30

def rotate_half(block, angle):
    half_dim = block.shape[-1] // 2
    cosine = jnp.cos(angle)[:, None, :]
    sine = jnp.sin(angle)[:, None, :]
    first = block[..., :half_dim]
    second = block[..., half_dim:]
    return jnp.concatenate([first * cosine - second * sine, second * cosine + first * sine], axis=-1)

def normalized_rotated(values_in, gain, heads, lattice_row, lattice_column):
    full = values_in.astype(jnp.float32).reshape(values_in.shape[0], heads, -1)
    full = full * lax.rsqrt(lax.optimization_barrier(jnp.mean(full * full, axis=-1, keepdims=True)) + EPS) * gain
    half_dim = full.shape[-1] // 2
    freqs = THETA ** (-2.0 * jnp.arange(half_dim // 2, dtype=jnp.float32) / half_dim)
    by_row = rotate_half(full[..., :half_dim], lattice_row[:, None] * freqs[None, :])
    by_col = rotate_half(full[..., half_dim:], lattice_column[:, None] * freqs[None, :])
    return jnp.concatenate([by_row, by_col], axis=-1).astype(jnp.bfloat16)

def reference(tokens_in, queries, keys, values, doc_ids, query_gain, key_norm_scale, out_weight, norm_gain, gate_weight, up_weight, down_weight):
    places = jnp.arange(PACKED_TOKENS, dtype=jnp.int32)
    lattice_row = (places // GRID).astype(jnp.float32)
    lattice_column = (places % GRID).astype(jnp.float32)
    q_all = normalized_rotated(queries, query_gain, QUERY_HEADS, lattice_row, lattice_column)
    every_key = normalized_rotated(keys, key_norm_scale, KEY_VALUE_HEADS, lattice_row, lattice_column).astype(jnp.float32)
    every_value = values.reshape(PACKED_TOKENS, KEY_VALUE_HEADS, HEAD_SIZE).astype(jnp.float32)
    query_group = QUERY_HEADS // KEY_VALUE_HEADS
    scale = HEAD_SIZE ** (-0.5)
    rows_per_block = 128

    def attend(start):
        query_tile = lax.dynamic_slice_in_dim(q_all, start, rows_per_block, 0).astype(jnp.float32)
        query_tile = query_tile.reshape(rows_per_block, KEY_VALUE_HEADS, query_group, HEAD_SIZE)
        doc_block = lax.dynamic_slice_in_dim(doc_ids, start, rows_per_block, 0)
        scores = jnp.einsum('qhgd,khd->hgqk', query_tile, every_key) * scale
        same = (doc_block[:, None] == doc_ids[None, :])[None, None]
        scores = jnp.where(same, scores, NEG)
        top = lax.optimization_barrier(jnp.max(scores, axis=-1, keepdims=True))
        weights = jnp.where(same, jnp.exp(scores - top), 0.0)
        total = lax.optimization_barrier(jnp.sum(weights, axis=-1))
        rounded = lax.optimization_barrier(weights.astype(jnp.bfloat16)).astype(jnp.float32)
        blended = jnp.einsum('hgqk,khd->hgqd', rounded, every_value) / total[..., None]
        return blended.transpose(2, 0, 1, 3).reshape(rows_per_block, QUERY_HEADS * HEAD_SIZE).astype(jnp.bfloat16)
    starts = jnp.arange(PACKED_TOKENS // rows_per_block, dtype=jnp.int32) * rows_per_block
    attended = lax.map(attend, starts).reshape(PACKED_TOKENS, QUERY_HEADS * HEAD_SIZE)
    share_cols = QUERY_HEADS * HEAD_SIZE // N_TP
    mixed = jnp.zeros((PACKED_TOKENS, D), jnp.float32)
    for member in range(N_TP):
        part_out = jnp.dot(attended[:, member * share_cols:(member + 1) * share_cols], out_weight[member * share_cols:(member + 1) * share_cols], preferred_element_type=jnp.float32)
        mixed = mixed + part_out.astype(jnp.bfloat16).astype(jnp.float32)
    resid = tokens_in.astype(jnp.float32) + mixed
    normed = (resid * lax.rsqrt(lax.optimization_barrier(jnp.mean(resid * resid, axis=-1, keepdims=True)) + EPS) * norm_gain).astype(jnp.bfloat16)
    gate = jnp.dot(normed, gate_weight, preferred_element_type=jnp.float32)
    up_val = jnp.dot(normed, up_weight, preferred_element_type=jnp.float32)
    hidden = (jax.nn.silu(gate) * up_val).astype(jnp.bfloat16)
    unit_cols = FF // N_TP
    fed = jnp.zeros((PACKED_TOKENS, D), jnp.float32)
    for member in range(N_TP):
        part_out = jnp.dot(hidden[:, member * unit_cols:(member + 1) * unit_cols], down_weight[member * unit_cols:(member + 1) * unit_cols], preferred_element_type=jnp.float32)
        fed = fed + part_out.astype(jnp.bfloat16).astype(jnp.float32)
    return (resid + fed).astype(jnp.bfloat16)
```

```python
import heapq
import jax
import jax.numpy as jnp
import numpy as np
from jax import lax
from jax.experimental import pallas as pl
from jax.experimental.pallas import tpu as pltpu
from jax.sharding import PartitionSpec as P

GRID = 64
EPS = 1e-06
THETA = 10000.0
NEG = -1e30
NZ, NY, NC, NX = 8, 4, 2, 4
DZS = (0, 1, -1, 2, -2, 3, -3, 4)
DYS = (0, 1, -1, 2)
MESH = pl.DeviceIdType.MESH
F32, BF16 = jnp.float32, jnp.bfloat16

PARTS = (
    ("k", "zy", 0.88, 0),
    ("v", "yz", 0.70, 0),
    ("g", "zy", 1.93, 1),
    ("u", "yz", 1.93, 1),
    ("a", "zy", 1.58, 2),
    ("b", "yz", 0.35, 2),
)


def spread(order, flip):
    messages = {}

    def z_ring(dy, up):
        for d in (1, 2, 3):
            messages[-d, dy] = ("z+", (-d + 1, dy))
            messages[d, dy] = ("z-", (d - 1, dy))
        messages[4, dy] = ("z+", (-3, dy)) if up else ("z-", (3, dy))

    def y_ring(dz, up):
        messages[dz, -1] = ("y+", (dz, 0))
        messages[dz, 1] = ("y-", (dz, 0))
        messages[dz, 2] = ("y+", (dz, -1)) if up else ("y-", (dz, 1))

    if order == "zy":
        z_ring(0, flip)
        for n, dz in enumerate(sorted(DZS)):
            y_ring(dz, (n + flip) % 2 == 0)
    else:
        y_ring(0, flip)
        for n, dy in enumerate(sorted(DYS)):
            z_ring(dy, (n + flip) % 2 == 0)
    return messages


def plan():
    received = {p[0]: spread(p[1], i % 2) for i, p in enumerate(PARTS)}
    cost = {p[0]: p[2] for p in PARTS}
    prio = {p[0]: p[3] for p in PARTS}
    follow = {}
    for part, messages in received.items():
        for key, (link, held) in messages.items():
            follow.setdefault((part, held), []).append((link, key))

    def depth(part, key):
        return max([1 + depth(part, k) for _, k in follow.get((part, key), [])], default=0)

    now, order = 0.0, []
    link_free = {link: 0.0 for link in ("z+", "z-", "y+", "y-", "d")}
    queues = {link: [] for link in link_free}
    arrivals = []
    have, sib = set(), set()
    latency, count = 2.0, 0

    def got(part, key):
        nonlocal count
        have.add((part, key))
        for link, k in follow.get((part, key), []):
            count += 1
            heapq.heappush(queues[link], (prio[part], -depth(part, k), count, part, k, key))
        dz = key[0]
        if all((part, (dz, dy)) in have for dy in DYS):
            order.append(("sib", part, dz))
            start = max(now, link_free["d"])
            link_free["d"] = start + 0.3
            count += 1
            heapq.heappush(arrivals, (start + 1.5, count, "sib", part, dz))

    def tick():
        nonlocal count
        while arrivals and arrivals[0][0] <= now:
            _, _, kind, part, key = heapq.heappop(arrivals)
            order.append(("wait" + kind, part, key))
            if kind == "sib":
                sib.add((part, key))
            else:
                got(part, key)
        for link in ("z+", "z-", "y+", "y-"):
            q = queues[link]
            while q and link_free[link] - now < 3.0:
                _, _, _, part, key, held = heapq.heappop(q)
                order.append(("send", part, key, held, link))
                start = max(now, link_free[link])
                link_free[link] = start + cost[part]
                count += 1
                heapq.heappush(arrivals, (link_free[link] + latency, count, "", part, key))

    def ready(step):
        kind = step[0]
        if kind == "attend":
            _, dz, own = step
            return all(((p, (dz, dy)) in have for p in "kv" for dy in DYS) if own else ((p, dz) in sib for p in "kv"))
        if kind == "gateup":
            return all((p, (dz, dy)) in have for p in "gu" for dz in DZS for dy in DYS) and all(
                (p, dz) in sib for p in "gu" for dz in DZS
            )
        if kind == "down":
            return all(
                all((p, (dz, dy)) in have for p in "ab" for dy in DYS) and all((p, dz) in sib for p in "ab")
                for dz in DZS[2 * step[1] : 2 * step[1] + 2]
            )
        return True

    steps = [("attend", dz, own) for dz in DZS for own in (True, False)]
    times = {"attend": 2.2, "attended": 1.0, "x_att": 2.5, "x_att2": 2.5, "mix": 1.0, "gateup": 0.9, "down": 0.8}
    steps += [("attended",), ("x_att",), ("x_att2",), ("mix", 0), ("mix", 1)]
    steps += [("gateup", n) for n in range(6)]
    steps += [("down", n) for n in range(4)]
    for part in "kvgu":
        got(part, (0, 0))
    tick()
    order.append(("more",))
    for part in "ab":
        got(part, (0, 0))
    for step in steps:
        tick()
        while not ready(step):
            now = max(now, arrivals[0][0])
            tick()
        order.append(step)
        now += times[step[0]]
    while arrivals:
        now = max(now, arrivals[0][0])
        tick()
    order.append(("end",))
    return order, now, link_free


def turn_tables():
    lane = np.arange(64)
    freqs = THETA ** (-2.0 * (lane % 16) / 32.0)
    sign = np.where(lane % 32 < 16, -1.0, 1.0)
    rows = np.arange(256)[:, None] * freqs[None]
    by_row = lane < 32
    row_cos = np.where(by_row, np.cos(rows), 0.0).reshape(64, 4, 64)
    row_sin = np.where(by_row, np.sin(rows) * sign, 0.0).reshape(64, 4, 64)
    row = np.concatenate([row_cos, row_sin], axis=1)
    cols = np.arange(64)[:, None] * freqs[None]
    col_cos = np.where(by_row, 0.0, np.cos(cols))
    col_sin = np.where(by_row, 0.0, np.sin(cols) * sign)
    col = np.stack([col_cos, col_sin])
    return np.tile(row, (1, 1, 2)).astype(np.float32), np.tile(col, (1, 1, 2)).astype(np.float32)


def nt(a, b):
    return lax.dot_general(a, b, (((1,), (1,)), ((), ())), preferred_element_type=F32)


def nn(a, b):
    return lax.dot_general(a, b, (((1,), (0,)), ((), ())), preferred_element_type=F32)


def kernel(
    tokens_ref,
    q_ref,
    k_ref,
    v_ref,
    doc_ref,
    gains_ref,
    ow_ref,
    ng_ref,
    gate_ref,
    up_ref,
    down_ref,
    row_ref,
    col_ref,
    out_ref,
    kt,
    vt,
    wg,
    wu,
    wa,
    wb,
    ow,
    att,
    qs,
    m_ref,
    l_ref,
    acc_ref,
    s_ref,
    p_ref,
    tok,
    resid,
    normed,
    hidden,
    part_buf,
    rs_buf,
    recv_sem,
    send_sem,
    sib_recv,
    sib_send,
    ow_recv,
    ow_send,
    ow_sib_recv,
    ow_sib_send,
    att_recv,
    att_send,
    rs_recv,
    rs_send,
    ag_recv,
    ag_send,
    local_sem,
):
    s = lax.axis_index("sp")
    x = lax.axis_index("tp")
    c = lax.rem(s, NC)
    y = lax.rem(s // NC, NY)
    z = s // (NC * NY)
    d = 1 - 2 * c

    def wz(dz):
        return lax.rem(z + (dz + NZ), NZ)

    def wy(dy):
        return lax.rem(y + (dy + NY), NY)

    def wx(dx):
        return lax.rem(x + (dx + NX), NX)

    def at(zz, yy, cc, xx):
        return ((zz * NY + yy) * NC + cc, xx)

    neighbour = {
        "z+": at(wz(1), y, c, x),
        "z-": at(wz(-1), y, c, x),
        "y+": at(z, wy(1), c, x),
        "y-": at(z, wy(-1), c, x),
    }
    sibling = at(z, y, 1 - c, x)
    x_plus = at(z, y, c, wx(1))
    x_minus = at(z, y, c, wx(-1))
    x_far = at(z, y, c, wx(2))
    x_f = at(z, y, c, wx(d))
    x_r = at(z, y, c, wx(-d))

    arrays = {"k": kt, "v": vt, "g": wg, "u": wu, "a": wa, "b": wb}
    names = [p[0] for p in PARTS]
    received = {p[0]: spread(p[1], i % 2) for i, p in enumerate(PARTS)}
    index = {name: {key: n for n, key in enumerate(received[name])} for name in names}

    local = [
        pltpu.make_async_copy(gate_ref, wg.at[z, y, c], local_sem.at[0]),
        pltpu.make_async_copy(up_ref, wu.at[z, y, c], local_sem.at[1]),
        pltpu.make_async_copy(ow_ref, ow.at[x], local_sem.at[2]),
        pltpu.make_async_copy(tokens_ref, tok, local_sem.at[3]),
    ]
    for copy in local:
        copy.start()

    barrier = pltpu.get_barrier_semaphore()
    for who in (*neighbour.values(), sibling, x_plus, x_minus, x_far):
        pl.semaphore_signal(barrier, inc=1, device_id=who, device_id_type=MESH)

    lane = lax.broadcasted_iota(jnp.int32, (256, 128), 1)
    low = lane < 64
    swap_up = lax.rem(lane // 16, 2) == 0
    row = row_ref[s]
    cos = jnp.concatenate([jnp.broadcast_to(row[r : r + 1], (64, 128)) + col_ref[0] for r in range(4)], axis=0)
    sin = jnp.concatenate([jnp.broadcast_to(row[r + 4 : r + 5], (64, 128)) + col_ref[1] for r in range(4)], axis=0)

    def turned(values, gain):
        square = values * values
        lo = jnp.sum(jnp.where(low, square, 0.0), axis=1, keepdims=True)
        hi = jnp.sum(jnp.where(low, 0.0, square), axis=1, keepdims=True)
        mean = jnp.where(low, lo, hi) * (1.0 / 64.0)
        values = values * lax.rsqrt(mean + EPS) * gain
        other = jnp.where(swap_up, pltpu.roll(values, 112, 1), pltpu.roll(values, 16, 1))
        return values * cos + other * sin

    def eye(n):
        return (
            lax.broadcasted_iota(jnp.int32, (n, n), 0) == lax.broadcasted_iota(jnp.int32, (n, n), 1)
        ).astype(F32).astype(BF16)

    kv = jnp.concatenate([k_ref[...], v_ref[...]], axis=1).astype(F32)
    kv = jnp.where(low, turned(kv, gains_ref[1:2]), kv).astype(BF16)
    kv_t = nt(eye(128), kv).astype(BF16)
    docs = jnp.broadcast_to(doc_ref[...], (16, 256))
    same = lax.broadcasted_iota(jnp.int32, (16, 256), 0) == docs
    kt[z, y, c, 0:64, :] = kv_t[:64]
    kt[z, y, c, 64:80, :] = jnp.where(same, NEG, 0.0).astype(BF16)
    vt[z, y, c] = kv_t[64:]

    pl.semaphore_wait(barrier, 8)

    def send(part, key, held, link):
        n = index[part][key]
        ref = arrays[part]
        slot = ref.at[wz(held[0]), wy(held[1]), c]
        i = names.index(part)
        which = 0 if n < 28 else 1
        return pltpu.make_async_remote_copy(
            src_ref=slot,
            dst_ref=slot,
            send_sem=send_sem.at[i, which],
            recv_sem=recv_sem.at[i, n],
            device_id=neighbour[link],
            device_id_type=MESH,
        )

    def wait_recv(part, key):
        n = index[part][key]
        i = names.index(part)
        slot = arrays[part].at[wz(key[0]), wy(key[1]), c]
        pltpu.make_async_remote_copy(
            src_ref=slot,
            dst_ref=slot,
            send_sem=send_sem.at[i, 0],
            recv_sem=recv_sem.at[i, n],
            device_id=sibling,
            device_id_type=MESH,
        ).wait_recv()

    def to_sibling(part, dz, cc):
        i = names.index(part)
        slots = arrays[part].at[wz(dz), :, cc]
        return pltpu.make_async_remote_copy(
            src_ref=slots,
            dst_ref=slots,
            send_sem=sib_send.at[i, DZS.index(dz)],
            recv_sem=sib_recv.at[i, DZS.index(dz)],
            device_id=sibling,
            device_id_type=MESH,
        )

    def half(member):
        return ow.at[member, pl.ds(pl.multiple_of(128 * c, 128), 128)]

    def ow_copy(member, n, who):
        return pltpu.make_async_remote_copy(
            src_ref=half(member),
            dst_ref=half(member),
            send_sem=ow_send.at[n],
            recv_sem=ow_recv.at[n],
            device_id=who,
            device_id_type=MESH,
        )

    def other_half(member, mine):
        cc = c if mine else 1 - c
        return ow.at[member, pl.ds(pl.multiple_of(128 * cc, 128), 128)]

    def ow_sib(member, n, mine):
        ref = other_half(member, mine)
        return pltpu.make_async_remote_copy(
            src_ref=ref,
            dst_ref=ref,
            send_sem=ow_sib_send.at[n],
            recv_sem=ow_sib_recv.at[n],
            device_id=sibling,
            device_id_type=MESH,
        )

    def att_copy(member, n, who):
        return pltpu.make_async_remote_copy(
            src_ref=att.at[member],
            dst_ref=att.at[member],
            send_sem=att_send.at[n],
            recv_sem=att_recv.at[n],
            device_id=who,
            device_id_type=MESH,
        )

    def rs_copy(j, member, n, who):
        return pltpu.make_async_remote_copy(
            src_ref=part_buf.at[j, member],
            dst_ref=rs_buf.at[j, n],
            send_sem=rs_send.at[j, n],
            recv_sem=rs_recv.at[j, n],
            device_id=who,
            device_id_type=MESH,
        )

    def out_chunk(member, dz):
        return out_ref.at[member, :, pl.ds(pl.multiple_of(256 * wz(dz), 256), 256)]

    def ag_copy(t, member, n, who):
        ref = out_chunk(member, DZS[t])
        return pltpu.make_async_remote_copy(
            src_ref=ref,
            dst_ref=ref,
            send_sem=ag_send.at[t, n],
            recv_sem=ag_recv.at[t, n],
            device_id=who,
            device_id_type=MESH,
        )

    def more():
        local[2].wait()
        ow_copy(x, 0, x_f).start()
        ow_copy(x, 1, x_r).start()
        no = jnp.where(same, 0.0, 1.0).astype(BF16)
        no = jnp.concatenate([jnp.zeros((64, 256), BF16), no, jnp.zeros((48, 256), BF16)], axis=0)
        no_t = nt(eye(256), no)
        for pair in range(2):
            both = turned(q_ref[:, 128 * pair : 128 * pair + 128].astype(F32), gains_ref[0:1]) * 0.125
            for odd in range(2):
                head = pltpu.roll(both, 64, 1) if odd else both
                qs[2 * pair + odd] = jnp.where(low, head, no_t).astype(BF16)
        m_ref[...] = jnp.full((4, 256, 128), NEG, F32)
        l_ref[...] = jnp.zeros((4, 256, 128), F32)
        acc_ref[...] = jnp.zeros((4, 256, 64), F32)
        down_t = nt(eye(32), down_ref[...]).astype(BF16)
        wa[z, y, c] = down_t[:, :1152]
        wb[z, y, c] = down_t[:, 1152:]

    def ow_forward():
        ow_copy(wx(-d), 0, x_f).wait_recv()
        ow_copy(wx(-d), 2, x_f).start()
        ow_sib(wx(-d), 0, True).start()
        ow_copy(wx(d), 1, x_r).wait_recv()
        ow_sib(wx(d), 1, True).start()

    def ow_last():
        ow_copy(wx(2), 2, x_f).wait_recv()
        ow_sib(wx(2), 2, True).start()

    def ow_wait():
        ow_sib(wx(d), 0, False).wait_recv()
        ow_sib(wx(-d), 1, False).wait_recv()
        ow_sib(wx(2), 2, False).wait_recv()

    def attend(dz, own):
        zz = wz(dz)
        cc = c if own else 1 - c

        def head(h, carry):
            q = qs[h][:, :80]
            for j in range(4):
                s_ref[:, 256 * j : 256 * j + 256] = nn(q, kt[zz, j, cc])
            for r in range(0, 256, 64):
                rows = slice(r, r + 64)
                sc = s_ref[rows, :]
                old = m_ref[h, rows, :]
                new = jnp.maximum(old, jnp.max(sc, axis=1, keepdims=True))
                shrink = jnp.exp(old - new)
                m_ref[h, rows, :] = new
                w = jnp.exp(sc - new[:, :1])
                part = w[:, :128]
                for t in range(1, 8):
                    part = part + w[:, 128 * t : 128 * t + 128]
                l_ref[h, rows, :] = l_ref[h, rows, :] * shrink + part
                acc_ref[h, rows, :] = acc_ref[h, rows, :] * shrink[:, :64]
                p_ref[rows, :] = w.astype(BF16)
            pv = nt(p_ref[:, 0:256], vt[zz, 0, cc])
            for j in range(1, 4):
                pv = pv + nt(p_ref[:, 256 * j : 256 * j + 256], vt[zz, j, cc])
            acc_ref[h] = acc_ref[h] + pv
            return carry

        lax.fori_loop(0, 4, head, 0)

    def attended():
        pieces = []
        for h in range(4):
            total = jnp.sum(l_ref[h], axis=1, keepdims=True)
            pieces.append(acc_ref[h] / total)
        att[x] = jnp.concatenate(pieces, axis=1).astype(BF16)
        att_copy(x, 0, x_f).start()
        att_copy(x, 1, x_r).start()

    def mix(n):
        if n == 0:
            att_copy(wx(2), 2, x_f).wait_recv()
            ow_wait()
            local[3].wait()
        rows = slice(128 * n, 128 * n + 128)
        total = tok[rows, :].astype(F32)
        mixed = jnp.zeros((128, 2048), F32)
        for member in range(4):
            mixed = mixed + nn(att[member, rows, :], ow[member]).astype(BF16).astype(F32)
        total = total + mixed
        resid[2 * n] = total[:64]
        resid[2 * n + 1] = total[64:]
        mean = jnp.mean(total * total, axis=1, keepdims=True)
        scaled = (total * lax.rsqrt(mean + EPS) * ng_ref[...]).astype(BF16)
        for t in range(8):
            normed[t, rows, :] = scaled[:, 256 * t : 256 * t + 256]

    def gateup(n):
        cols = slice(256 * n, min(256 * n + 256, 1408))
        width = cols.stop - cols.start
        gate = jnp.zeros((256, width), F32)
        up = jnp.zeros((256, width), F32)
        for t in range(8):
            a = normed[t]
            gate = gate + nn(a, wg[t, :, :, :, cols].reshape(256, width))
            up = up + nn(a, wu[t, :, :, :, cols].reshape(256, width))
        hidden[:, cols] = (gate / (1.0 + jnp.exp(-gate)) * up).astype(BF16)

    def down(j):
        for t in range(2):
            zz = wz(DZS[2 * j + t])
            fed = nt(hidden[:, :1152], wa[zz].reshape(256, 1152)) + nt(hidden[:, 1152:], wb[zz].reshape(256, 256))
            fed = fed.astype(BF16)
            for member in range(4):
                part_buf[j, member, :, 256 * t : 256 * t + 256] = fed[64 * member : 64 * member + 64]
        rs_copy(j, wx(2), 2, x_far).start()
        rs_copy(j, wx(1), 0, x_plus).start()
        rs_copy(j, wx(-1), 1, x_minus).start()

    def reduce(j):
        rs_copy(j, wx(1), 0, x_plus).wait_recv()
        rs_copy(j, wx(-1), 1, x_minus).wait_recv()
        rs_copy(j, wx(2), 2, x_far).wait_recv()
        total = part_buf[j, x].astype(F32)
        for n in range(3):
            total = total + rs_buf[j, n].astype(F32)
        for t in range(2):
            zz = wz(DZS[2 * j + t])
            cols = pl.ds(pl.multiple_of(256 * zz, 256), 256)
            out_ref[x, :, cols] = (resid[x, :, cols] + total[:, 256 * t : 256 * t + 256]).astype(BF16)
            ag_copy(2 * j + t, x, 0, x_f).start()
            ag_copy(2 * j + t, x, 1, x_r).start()

    def relay(j):
        for t in (2 * j, 2 * j + 1):
            ag_copy(t, wx(-d), 0, x_f).wait_recv()
            ag_copy(t, wx(-d), 2, x_f).start()

    def end():
        for i, name in enumerate(names):
            ref = arrays[name]
            many = ref.at[0:7, :, 0]
            few = ref.at[0, 0:3, 0]
            pltpu.make_async_remote_copy(
                src_ref=many,
                dst_ref=many,
                send_sem=send_sem.at[i, 0],
                recv_sem=recv_sem.at[i, 0],
                device_id=sibling,
                device_id_type=MESH,
            ).wait_send()
            pltpu.make_async_remote_copy(
                src_ref=few,
                dst_ref=few,
                send_sem=send_sem.at[i, 1],
                recv_sem=recv_sem.at[i, 0],
                device_id=sibling,
                device_id_type=MESH,
            ).wait_send()
            for dz in DZS:
                to_sibling(name, dz, c).wait_send()
        ow_copy(x, 0, x_f).wait_send()
        ow_copy(x, 1, x_r).wait_send()
        ow_copy(wx(-d), 2, x_f).wait_send()
        for n, member in enumerate((wx(-d), wx(d), wx(2))):
            ow_sib(member, n, True).wait_send()
        att_copy(x, 0, x_f).wait_send()
        att_copy(x, 1, x_r).wait_send()
        att_copy(wx(-d), 2, x_f).wait_send()
        for j in range(4):
            rs_copy(j, wx(2), 2, x_far).wait_send()
            rs_copy(j, wx(1), 0, x_plus).wait_send()
            rs_copy(j, wx(-1), 1, x_minus).wait_send()
        for t in range(8):
            ag_copy(t, wx(d), 1, x_r).wait_recv()
            ag_copy(t, wx(2), 2, x_f).wait_recv()
            ag_copy(t, x, 0, x_f).wait_send()
            ag_copy(t, x, 1, x_r).wait_send()
            ag_copy(t, wx(-d), 2, x_f).wait_send()

    order, _, _ = plan()
    local_left = True
    groups = 0
    for event in order:
        kind = event[0]
        if kind == "send":
            _, part, key, held, link = event
            if part in "gu" and local_left:
                local[0].wait()
                local[1].wait()
                local_left = False
            send(part, key, held, link).start()
        elif kind == "wait":
            wait_recv(event[1], event[2])
        elif kind == "sib":
            to_sibling(event[1], event[2], c).start()
        elif kind == "waitsib":
            to_sibling(event[1], event[2], 1 - c).wait_recv()
        elif kind == "more":
            more()
        elif kind == "attend":
            attend(event[1], event[2])
            groups += 1
            if groups == 7:
                ow_forward()
            if groups == 14:
                ow_last()
        elif kind == "attended":
            attended()
        elif kind == "x_att":
            att_copy(wx(-d), 0, x_f).wait_recv()
            att_copy(wx(-d), 2, x_f).start()
            att_copy(wx(d), 1, x_r).wait_recv()
        elif kind == "mix":
            mix(event[1])
        elif kind == "gateup":
            gateup(event[1])
        elif kind == "down":
            j = event[1]
            down(j)
            if j >= 1:
                reduce(j - 1)
            if j >= 2:
                relay(j - 2)
        elif kind == "end":
            reduce(3)
            relay(2)
            relay(3)
            end()


def per_device(
    tokens_in,
    queries,
    keys,
    values,
    doc_ids,
    query_gain,
    key_norm_scale,
    out_weight,
    norm_gain,
    gate_weight,
    up_weight,
    down_weight,
):
    row, col = turn_tables()
    gains = jnp.stack([jnp.tile(query_gain, 2), jnp.tile(key_norm_scale, 2)])
    vmem = pl.BlockSpec(memory_space=pltpu.VMEM)
    hbm = pl.BlockSpec(memory_space=pl.ANY)
    dma = pltpu.SemaphoreType.DMA
    out = pl.pallas_call(
        kernel,
        name="layer",
        out_shape=jax.ShapeDtypeStruct((4, 64, 2048), BF16),
        in_specs=[hbm, vmem, vmem, vmem, vmem, vmem, hbm, vmem, hbm, hbm, vmem, vmem, vmem],
        out_specs=vmem,
        scratch_shapes=[
            pltpu.VMEM((NZ, NY, NC, 80, 256), BF16),
            pltpu.VMEM((NZ, NY, NC, 64, 256), BF16),
            pltpu.VMEM((NZ, NY, NC, 32, 1408), BF16),
            pltpu.VMEM((NZ, NY, NC, 32, 1408), BF16),
            pltpu.VMEM((NZ, NY, NC, 32, 1152), BF16),
            pltpu.VMEM((NZ, NY, NC, 32, 256), BF16),
            pltpu.VMEM((4, 256, 2048), BF16),
            pltpu.VMEM((4, 256, 256), BF16),
            pltpu.VMEM((4, 256, 128), BF16),
            pltpu.VMEM((4, 256, 128), F32),
            pltpu.VMEM((4, 256, 128), F32),
            pltpu.VMEM((4, 256, 64), F32),
            pltpu.VMEM((256, 1024), F32),
            pltpu.VMEM((256, 1024), BF16),
            pltpu.VMEM((256, 2048), BF16),
            pltpu.VMEM((4, 64, 2048), F32),
            pltpu.VMEM((8, 256, 256), BF16),
            pltpu.VMEM((256, 1408), BF16),
            pltpu.VMEM((4, 4, 64, 512), BF16),
            pltpu.VMEM((4, 3, 64, 512), BF16),
            dma((6, 31)),
            dma((6, 2)),
            dma((6, 8)),
            dma((6, 8)),
            dma((3,)),
            dma((3,)),
            dma((3,)),
            dma((3,)),
            dma((3,)),
            dma((3,)),
            dma((4, 3)),
            dma((4, 3)),
            dma((8, 3)),
            dma((8, 3)),
            dma((4,)),
        ],
        compiler_params=pltpu.CompilerParams(
            collective_id=0, has_side_effects=True, vmem_limit_bytes=60 * 1024 * 1024
        ),
    )(
        tokens_in,
        queries,
        keys,
        values,
        doc_ids.reshape(1, -1),
        gains,
        out_weight,
        norm_gain.reshape(1, -1),
        gate_weight,
        up_weight,
        down_weight,
        jnp.asarray(row),
        jnp.asarray(col),
    )
    return out.reshape(256, 2048)


def solution(mesh):
    return jax.shard_map(
        per_device,
        mesh=mesh,
        in_specs=(
            P("sp", None),
            P("sp", "tp"),
            P("sp", "tp"),
            P("sp", "tp"),
            P("sp"),
            P(),
            P(),
            P("tp", None),
            P(),
            P("sp", "tp"),
            P("sp", "tp"),
            P("tp", "sp"),
        ),
        out_specs=P("sp", None),
        check_vma=False,
    )
```

```python
import heapq
import jax
import jax.numpy as jnp
import numpy as np
from jax import lax
from jax.experimental import pallas as pl
from jax.experimental.pallas import tpu as pltpu
from jax.sharding import PartitionSpec as P

GRID = 64
EPS = 1e-06
THETA = 10000.0
NEG = -1e30
NZ, NY, NC, NX = 8, 4, 2, 4
DZS = (0, 1, -1, 2, -2, 3, -3, 4)
DYS = (0, 1, -1, 2)
MESH = pl.DeviceIdType.MESH
F32, BF16 = jnp.float32, jnp.bfloat16

DOWN_A = 768
PARTS = (
    ("k", "zy", 1, 0.88, -37.1),
    ("v", "yz", 0, 0.70, 19.9),
    ("g", "zy", 1, 1.93, 78.0),
    ("u", "yz", 0, 1.93, 73.8),
    ("a", "zy", 0, 1.93 * 6 / 11, 96.9),
    ("b", "yz", 0, 1.93 * 5 / 11, 101.0),
)
HOP = 4.4
BACKLOG = 2.0
LATENCY = 2.4


def spread(order, flip):
    messages = {}

    def z_ring(dy, up):
        for d in (1, 2, 3):
            messages[-d, dy] = ("z+", (-d + 1, dy))
            messages[d, dy] = ("z-", (d - 1, dy))
        messages[4, dy] = ("z+", (-3, dy)) if up else ("z-", (3, dy))

    def y_ring(dz, up):
        messages[dz, -1] = ("y+", (dz, 0))
        messages[dz, 1] = ("y-", (dz, 0))
        messages[dz, 2] = ("y+", (dz, -1)) if up else ("y-", (dz, 1))

    if order == "zy":
        z_ring(0, flip)
        for n, dz in enumerate(sorted(DZS)):
            y_ring(dz, (n + flip) % 2 == 0)
    else:
        y_ring(0, flip)
        for n, dy in enumerate(sorted(DYS)):
            z_ring(dy, (n + flip) % 2 == 0)
    return messages


def plan():
    received = {p[0]: spread(p[1], p[2]) for p in PARTS}
    cost = {p[0]: p[3] for p in PARTS}
    due = {p[0]: p[4] for p in PARTS}
    times = {"attend": 2.0, "attended": 0.4, "mix": 1.0, "gateup": 0.78, "down": 0.4, "reduce": 0.2}
    follow = {}
    for part, messages in received.items():
        for key, (link, held) in messages.items():
            follow.setdefault((part, held), []).append((link, key))

    def depth(part, key):
        return max([1 + depth(part, k) for _, k in follow.get((part, key), [])], default=0)

    now, count, order = 0.0, 0, []
    link_free = {link: 0.0 for link in ("z+", "z-", "y+", "y-", "d", "x")}
    queues = {link: [] for link in ("z+", "z-", "y+", "y-")}
    arrivals = []
    have, sib, done = set(), set(), set()

    def push(when, *event):
        nonlocal count
        count += 1
        heapq.heappush(arrivals, (when, count) + event)

    def got(part, key):
        nonlocal count
        have.add((part, key))
        for link, k in follow.get((part, key), []):
            count += 1
            heapq.heappush(queues[link], (due[part] - depth(part, k) * (cost[part] + HOP), count, part, k, key))
        dz = key[0]
        if all((part, (dz, dy)) in have for dy in DYS):
            order.append(("sib", part, dz))
            start = max(now, link_free["d"])
            link_free["d"] = start + 0.3
            push(start + 1.5, "sib", part, dz)

    def tick():
        while arrivals and arrivals[0][0] <= now:
            _, _, kind, part, key = heapq.heappop(arrivals)
            order.append(("wait" + kind, part, key))
            if kind == "sib":
                sib.add((part, key))
            elif kind == "":
                got(part, key)
            else:
                done.add((kind, part))
        for link, queue in queues.items():
            while queue and link_free[link] - now < BACKLOG:
                _, _, part, key, held = heapq.heappop(queue)
                order.append(("send", part, key, held, link))
                link_free[link] = max(now, link_free[link]) + cost[part]
                push(link_free[link] + LATENCY, "", part, key)

    def near(parts, dz):
        return all((p, (dz, dy)) in have for p in parts for dy in DYS)

    def ready(step):
        kind = step[0]
        if kind == "attend":
            return near("kv", step[1]) if step[2] else all((p, step[1]) in sib for p in "kv")
        if kind == "gateup":
            return all(near("gu", dz) and all((p, dz) in sib for p in "gu") for dz in DZS)
        if kind == "mix":
            return ("att", 0) in done
        if kind == "down":
            return near("ab", step[1]) and all((p, step[1]) in sib for p in "ab")
        if kind == "reduce":
            return ("rs", step[1]) in done
        return True

    def run(step):
        nonlocal now
        order.append(step)
        now += times[step[0]]
        sends = {"attended": ("att", 5.0), "down": ("rs", 1.4), "reduce": ("ag", 1.4)}
        if step[0] in sends:
            kind, length = sends[step[0]]
            link_free["x"] = max(now, link_free["x"]) + length
            push(link_free["x"] + LATENCY, kind, step[1], 0)

    def advance():
        nonlocal now
        now = max(now, arrivals[0][0])
        tick()

    for part in "kvgu":
        got(part, (0, 0))
    tick()
    order.append(("more",))
    for part in "ab":
        got(part, (0, 0))
    now = 0.75
    steps = [("attend", dz, own) for dz in DZS for own in (True, False)]
    steps += [("attended", 0), ("mix", 0), ("mix", 1)]
    steps += [("gateup", n) for n in range(6)]
    for step in steps:
        tick()
        while not ready(step):
            advance()
        run(step)
    downs, reduces = list(DZS), []
    while downs or reduces:
        tick()
        steps = [("reduce", dz) for dz in reduces] + [("down", dz) for dz in downs]
        step = next((step for step in steps if ready(step)), None)
        if step is None:
            advance()
            continue
        run(step)
        if step[0] == "down":
            downs.remove(step[1])
            reduces.append(step[1])
        else:
            reduces.remove(step[1])
    while arrivals:
        advance()
    order.append(("end",))
    return order, now


def turn_tables():
    lane = np.arange(64)
    freqs = THETA ** (-2.0 * (lane % 16) / 32.0)
    sign = np.where(lane % 32 < 16, -1.0, 1.0)
    rows = np.arange(256)[:, None] * freqs[None]
    by_row = lane < 32
    row_cos = np.where(by_row, np.cos(rows), 0.0).reshape(64, 4, 64)
    row_sin = np.where(by_row, np.sin(rows) * sign, 0.0).reshape(64, 4, 64)
    row = np.concatenate([row_cos, row_sin], axis=1)
    cols = np.arange(64)[:, None] * freqs[None]
    col_cos = np.where(by_row, 0.0, np.cos(cols))
    col_sin = np.where(by_row, 0.0, np.sin(cols) * sign)
    col = np.stack([col_cos, col_sin])
    return np.tile(row, (1, 1, 2)).astype(np.float32), np.tile(col, (1, 1, 2)).astype(np.float32)


def nt(a, b):
    return lax.dot_general(a, b, (((1,), (1,)), ((), ())), preferred_element_type=F32)


def nn(a, b):
    return lax.dot_general(a, b, (((1,), (0,)), ((), ())), preferred_element_type=F32)


def kernel(
    tokens_ref,
    q_ref,
    k_ref,
    v_ref,
    doc_ref,
    qg_ref,
    kg_ref,
    ow_ref,
    ng_ref,
    gate_ref,
    up_ref,
    down_ref,
    row_ref,
    col_ref,
    out_ref,
    kt,
    vt,
    wg,
    wu,
    wa,
    wb,
    ow,
    att,
    qs,
    m_ref,
    l_ref,
    acc_ref,
    s_ref,
    p_ref,
    tok,
    resid,
    normed,
    hidden,
    part_buf,
    rs_buf,
    recv_sem,
    send_sem,
    sib_recv,
    sib_send,
    ow_recv,
    ow_send,
    ow_sib_recv,
    ow_sib_send,
    att_recv,
    att_send,
    rs_recv,
    rs_send,
    ag_recv,
    ag_send,
    local_sem,
):
    s = lax.axis_index("sp")
    x = lax.axis_index("tp")
    c = lax.rem(s, NC)
    y = lax.rem(s // NC, NY)
    z = s // (NC * NY)

    def wz(dz):
        return lax.rem(z + (dz + NZ), NZ)

    def wy(dy):
        return lax.rem(y + (dy + NY), NY)

    def wx(dx):
        return lax.rem(x + (dx + NX), NX)

    def at(zz, yy, cc, xx):
        return ((zz * NY + yy) * NC + cc, xx)

    neighbour = {
        "z+": at(wz(1), y, c, x),
        "z-": at(wz(-1), y, c, x),
        "y+": at(z, wy(1), c, x),
        "y-": at(z, wy(-1), c, x),
    }
    sibling = at(z, y, 1 - c, x)
    x_plus = at(z, y, c, wx(1))
    x_minus = at(z, y, c, wx(-1))
    x_far = at(z, y, c, wx(2))

    arrays = {"k": kt, "v": vt, "g": wg, "u": wu, "a": wa, "b": wb}
    names = [p[0] for p in PARTS]
    received = {p[0]: spread(p[1], p[2]) for p in PARTS}
    index = {name: {key: n for n, key in enumerate(received[name])} for name in names}

    local = [
        pltpu.make_async_copy(v_ref, vt.at[z, y, c], local_sem.at[0]),
        pltpu.make_async_copy(gate_ref, wg.at[z, y, c], local_sem.at[1]),
        pltpu.make_async_copy(up_ref, wu.at[z, y, c], local_sem.at[2]),
        pltpu.make_async_copy(down_ref.at[:, :DOWN_A], wa.at[z, y, c], local_sem.at[3]),
        pltpu.make_async_copy(down_ref.at[:, DOWN_A:], wb.at[z, y, c], local_sem.at[4]),
        pltpu.make_async_copy(ow_ref, ow.at[x], local_sem.at[5]),
        pltpu.make_async_copy(tokens_ref, tok, local_sem.at[6]),
    ]
    for copy in local:
        copy.start()

    barrier = pltpu.get_barrier_semaphore()
    for who in (*neighbour.values(), sibling, x_plus, x_minus, x_far):
        pl.semaphore_signal(barrier, inc=1, device_id=who, device_id_type=MESH)

    lane = lax.broadcasted_iota(jnp.int32, (256, 128), 1)
    low = lane < 64
    swap_up = lax.rem(lane // 16, 2) == 0
    row = row_ref[s]
    cos = jnp.concatenate([jnp.broadcast_to(row[r : r + 1], (64, 128)) + col_ref[0] for r in range(4)], axis=0)
    sin = jnp.concatenate([jnp.broadcast_to(row[r + 4 : r + 5], (64, 128)) + col_ref[1] for r in range(4)], axis=0)

    def turned(values, gain):
        square = values * values
        lo = jnp.sum(jnp.where(low, square, 0.0), axis=1, keepdims=True)
        hi = jnp.sum(jnp.where(low, 0.0, square), axis=1, keepdims=True)
        mean = jnp.where(low, lo, hi) * (1.0 / 64.0)
        values = values * lax.rsqrt(mean + EPS) * gain
        other = jnp.where(swap_up, pltpu.roll(values, 112, 1), pltpu.roll(values, 16, 1))
        return values * cos + other * sin

    def eye(n):
        return (
            lax.broadcasted_iota(jnp.int32, (n, n), 0) == lax.broadcasted_iota(jnp.int32, (n, n), 1)
        ).astype(F32).astype(BF16)

    keys = k_ref[...].astype(F32)
    gain = jnp.where(
        lax.broadcasted_iota(jnp.int32, (64, 64), 0) == lax.broadcasted_iota(jnp.int32, (64, 64), 1), kg_ref[...], 0.0
    )
    keys = keys * lax.rsqrt(jnp.mean(keys * keys, axis=0, keepdims=True) + EPS) * jnp.sum(gain, axis=1, keepdims=True)
    other = jnp.concatenate([keys[16:32], keys[0:16], keys[48:64], keys[32:48]], axis=0)
    keys = keys * jnp.transpose(cos)[:64] + other * jnp.transpose(sin)[:64]
    docs = jnp.broadcast_to(doc_ref[...], (16, 256))
    same = lax.broadcasted_iota(jnp.int32, (16, 256), 0) == docs
    kt[z, y, c, 0:64, :] = keys.astype(BF16)
    kt[z, y, c, 64:80, :] = jnp.where(same, NEG, 0.0).astype(BF16)
    local[0].wait()

    pl.semaphore_wait(barrier, 8)

    def send(part, key, held, link):
        n = index[part][key]
        ref = arrays[part]
        slot = ref.at[wz(held[0]), wy(held[1]), c]
        i = names.index(part)
        which = 0 if n < 28 else 1
        return pltpu.make_async_remote_copy(
            src_ref=slot,
            dst_ref=slot,
            send_sem=send_sem.at[i, which],
            recv_sem=recv_sem.at[i, n],
            device_id=neighbour[link],
            device_id_type=MESH,
        )

    def wait_recv(part, key):
        n = index[part][key]
        i = names.index(part)
        slot = arrays[part].at[wz(key[0]), wy(key[1]), c]
        pltpu.make_async_remote_copy(
            src_ref=slot,
            dst_ref=slot,
            send_sem=send_sem.at[i, 0],
            recv_sem=recv_sem.at[i, n],
            device_id=sibling,
            device_id_type=MESH,
        ).wait_recv()

    def to_sibling(part, dz, cc):
        i = names.index(part)
        slots = arrays[part].at[wz(dz), :, cc]
        return pltpu.make_async_remote_copy(
            src_ref=slots,
            dst_ref=slots,
            send_sem=sib_send.at[i, DZS.index(dz)],
            recv_sem=sib_recv.at[i, DZS.index(dz)],
            device_id=sibling,
            device_id_type=MESH,
        )

    def half(member):
        return ow.at[member, pl.ds(pl.multiple_of(128 * c, 128), 128)]

    def ow_copy(member, n, who):
        return pltpu.make_async_remote_copy(
            src_ref=half(member),
            dst_ref=half(member),
            send_sem=ow_send.at[n],
            recv_sem=ow_recv.at[n],
            device_id=who,
            device_id_type=MESH,
        )

    def other_half(member, mine):
        cc = c if mine else 1 - c
        return ow.at[member, pl.ds(pl.multiple_of(128 * cc, 128), 128)]

    def ow_sib(member, n, mine):
        ref = other_half(member, mine)
        return pltpu.make_async_remote_copy(
            src_ref=ref,
            dst_ref=ref,
            send_sem=ow_sib_send.at[n],
            recv_sem=ow_sib_recv.at[n],
            device_id=sibling,
            device_id_type=MESH,
        )

    def att_copy(member, n, who):
        return pltpu.make_async_remote_copy(
            src_ref=att.at[member],
            dst_ref=att.at[member],
            send_sem=att_send.at[n],
            recv_sem=att_recv.at[n],
            device_id=who,
            device_id_type=MESH,
        )

    def rs_copy(j, member, n, who):
        return pltpu.make_async_remote_copy(
            src_ref=part_buf.at[j, member],
            dst_ref=rs_buf.at[j, n],
            send_sem=rs_send.at[j, n],
            recv_sem=rs_recv.at[j, n],
            device_id=who,
            device_id_type=MESH,
        )

    def out_chunk(member, dz):
        return out_ref.at[member, :, pl.ds(pl.multiple_of(256 * wz(dz), 256), 256)]

    def ag_copy(t, member, n, who):
        ref = out_chunk(member, DZS[t])
        return pltpu.make_async_remote_copy(
            src_ref=ref,
            dst_ref=ref,
            send_sem=ag_send.at[t, n],
            recv_sem=ag_recv.at[t, n],
            device_id=who,
            device_id_type=MESH,
        )

    def more():
        local[5].wait()
        ow_copy(x, 2, x_far).start()
        ow_copy(x, 0, x_plus).start()
        ow_copy(x, 1, x_minus).start()
        no = jnp.where(same, 0.0, 1.0).astype(BF16)
        no = jnp.concatenate([jnp.zeros((64, 256), BF16), no, jnp.zeros((48, 256), BF16)], axis=0)
        no_t = nt(eye(256), no)
        query_gain = jnp.concatenate([qg_ref[...], qg_ref[...]], axis=1)
        for pair in range(2):
            both = turned(q_ref[:, 128 * pair : 128 * pair + 128].astype(F32), query_gain) * 0.125
            for odd in range(2):
                head = pltpu.roll(both, 64, 1) if odd else both
                qs[2 * pair + odd] = jnp.where(low, head, no_t).astype(BF16)
        m_ref[...] = jnp.full((4, 256, 128), NEG, F32)
        l_ref[...] = jnp.zeros((4, 256, 128), F32)
        acc_ref[...] = jnp.zeros((4, 256, 64), F32)
        local[3].wait()
        local[4].wait()

    def ow_forward():
        for n, member in enumerate((wx(-1), wx(1), wx(2))):
            ow_copy(member, n, x_far).wait_recv()
            ow_sib(member, n, True).start()

    def ow_wait():
        for n, member in enumerate((wx(-1), wx(1), wx(2))):
            ow_sib(member, n, False).wait_recv()

    def attend(i):
        n = i // 2
        zz = wz((n + 1) // 2 * (2 * lax.rem(n, 2) - 1))
        cc = lax.rem(c + i, 2)

        def scores(h):
            q = qs[h][:, :80]
            for j in range(4):
                s_ref[h % 2, :, 256 * j : 256 * j + 256] = nn(q, kt[zz, j, cc])

        scores(0)
        for h in range(4):
            if h < 3:
                scores(h + 1)
            for r in range(0, 256, 32):
                rows = slice(r, r + 32)
                sc = s_ref[h % 2, rows, :]
                old = m_ref[h, rows, :]
                new = jnp.maximum(old, jnp.max(sc, axis=1, keepdims=True))
                shrink = jnp.exp(old - new)
                m_ref[h, rows, :] = new
                w = jnp.exp(sc - new[:, :1])
                part = w[:, :128]
                for t in range(1, 8):
                    part = part + w[:, 128 * t : 128 * t + 128]
                l_ref[h, rows, :] = l_ref[h, rows, :] * shrink + part
                acc_ref[h, rows, :] = acc_ref[h, rows, :] * shrink[:, :64]
                p_ref[h % 2, rows, :] = w.astype(BF16)
            pv = nt(p_ref[h % 2, :, 0:256], vt[zz, 0, cc])
            for j in range(1, 4):
                pv = pv + nt(p_ref[h % 2, :, 256 * j : 256 * j + 256], vt[zz, j, cc])
            acc_ref[h] = acc_ref[h] + pv

    def attended():
        pieces = []
        for h in range(4):
            total = jnp.sum(l_ref[h], axis=1, keepdims=True)
            pieces.append(acc_ref[h] / total)
        att[x] = jnp.concatenate(pieces, axis=1).astype(BF16)
        att_copy(x, 2, x_far).start()
        att_copy(x, 0, x_plus).start()
        att_copy(x, 1, x_minus).start()

    def mix(n):
        if n == 0:
            ow_wait()
            local[6].wait()
        rows = slice(128 * n, 128 * n + 128)
        total = tok[rows, :].astype(F32)
        mixed = jnp.zeros((128, 2048), F32)
        for member in range(4):
            mixed = mixed + nn(att[member, rows, :], ow[member]).astype(BF16).astype(F32)
        total = total + mixed
        resid[2 * n] = total[:64]
        resid[2 * n + 1] = total[64:]
        mean = jnp.mean(total * total, axis=1, keepdims=True)
        scaled = (total * lax.rsqrt(mean + EPS) * ng_ref[...]).astype(BF16)
        for t in range(8):
            normed[t, rows, :] = scaled[:, 256 * t : 256 * t + 256]

    def gateup(n):
        cols = slice(256 * n, min(256 * n + 256, 1408))
        width = cols.stop - cols.start
        gate = jnp.zeros((256, width), F32)
        up = jnp.zeros((256, width), F32)
        for t in range(8):
            a = normed[t]
            gate = gate + nn(a, wg[t, :, :, :, cols].reshape(256, width))
            up = up + nn(a, wu[t, :, :, :, cols].reshape(256, width))
        hidden[:, cols] = (gate / (1.0 + jnp.exp(-gate)) * up).astype(BF16)

    def down(dz):
        j = DZS.index(dz)
        zz = wz(dz)
        fed = nt(hidden[:, :DOWN_A], wa[zz].reshape(256, DOWN_A))
        fed = (fed + nt(hidden[:, DOWN_A:], wb[zz].reshape(256, 1408 - DOWN_A))).astype(BF16)
        for member in range(4):
            part_buf[j, member] = fed[64 * member : 64 * member + 64]
        rs_copy(j, wx(2), 2, x_far).start()
        rs_copy(j, wx(1), 0, x_plus).start()
        rs_copy(j, wx(-1), 1, x_minus).start()

    def wait_rs(dz):
        j = DZS.index(dz)
        for n in range(3):
            rs_copy(j, x, n, x_far).wait_recv()

    def reduce(dz):
        j = DZS.index(dz)
        total = part_buf[j, x].astype(F32)
        for n in range(3):
            total = total + rs_buf[j, n].astype(F32)
        cols = pl.ds(pl.multiple_of(256 * wz(dz), 256), 256)
        out_ref[x, :, cols] = (resid[x, :, cols] + total).astype(BF16)
        ag_copy(j, x, 2, x_far).start()
        ag_copy(j, x, 0, x_plus).start()
        ag_copy(j, x, 1, x_minus).start()

    def wait_ag(dz):
        j = DZS.index(dz)
        for n, member in enumerate((wx(-1), wx(1), wx(2))):
            ag_copy(j, member, n, x_far).wait_recv()

    def end():
        for i, name in enumerate(names):
            ref = arrays[name]
            many = ref.at[0:7, :, 0]
            few = ref.at[0, 0:3, 0]
            pltpu.make_async_remote_copy(
                src_ref=many,
                dst_ref=many,
                send_sem=send_sem.at[i, 0],
                recv_sem=recv_sem.at[i, 0],
                device_id=sibling,
                device_id_type=MESH,
            ).wait_send()
            pltpu.make_async_remote_copy(
                src_ref=few,
                dst_ref=few,
                send_sem=send_sem.at[i, 1],
                recv_sem=recv_sem.at[i, 0],
                device_id=sibling,
                device_id_type=MESH,
            ).wait_send()
            for dz in DZS:
                to_sibling(name, dz, c).wait_send()
        for n, who in enumerate((x_plus, x_minus, x_far)):
            ow_copy(x, n, who).wait_send()
            att_copy(x, n, who).wait_send()
        for n, member in enumerate((wx(-1), wx(1), wx(2))):
            ow_sib(member, n, True).wait_send()
        for j in range(8):
            for n, (who, member) in enumerate(((x_plus, wx(1)), (x_minus, wx(-1)), (x_far, wx(2)))):
                rs_copy(j, member, n, who).wait_send()
                ag_copy(j, x, n, who).wait_send()

    done = set()

    def handle(event):
        kind = event[0]
        if kind == "send":
            _, part, key, held, link = event
            if part in "gu" and part not in done:
                local[1 + "gu".index(part)].wait()
                done.add(part)
            send(part, key, held, link).start()
        elif kind == "wait":
            wait_recv(event[1], event[2])
        elif kind == "sib":
            to_sibling(event[1], event[2], c).start()
        elif kind == "waitsib":
            to_sibling(event[1], event[2], 1 - c).wait_recv()
        elif kind == "more":
            more()
        elif kind == "attended":
            attended()
        elif kind == "waitatt":
            for n, member in enumerate((wx(-1), wx(1), wx(2))):
                att_copy(member, n, x_far).wait_recv()
        elif kind == "mix":
            mix(event[1])
        elif kind == "gateup":
            gateup(event[1])
        elif kind == "down":
            down(event[1])
        elif kind == "waitrs":
            wait_rs(event[1])
        elif kind == "reduce":
            reduce(event[1])
        elif kind == "waitag":
            wait_ag(event[1])
        elif kind == "end":
            end()

    order, _ = plan()
    attends = [n for n, event in enumerate(order) if event[0] == "attend"]
    for event in order[: attends[0]]:
        handle(event)

    def step(i, carry):
        attend(i)
        for n in range(16):
            stop = attends[n + 1] if n < 15 else attends[15] + 1

            @pl.when(i == n)
            def _():
                for event in order[attends[n] + 1 : stop]:
                    handle(event)
                if n == 11:
                    ow_forward()

        return carry

    lax.fori_loop(0, 16, step, 0)
    for event in order[attends[15] + 1 :]:
        handle(event)


def per_device(
    tokens_in,
    queries,
    keys,
    values,
    doc_ids,
    query_gain,
    key_norm_scale,
    out_weight,
    norm_gain,
    gate_weight,
    up_weight,
    down_weight,
):
    row, col = turn_tables()
    vmem = pl.BlockSpec(memory_space=pltpu.VMEM)
    hbm = pl.BlockSpec(memory_space=pl.ANY)
    dma = pltpu.SemaphoreType.DMA
    out = pl.pallas_call(
        kernel,
        name="layer",
        out_shape=jax.ShapeDtypeStruct((4, 64, 2048), BF16),
        in_specs=[hbm, vmem, vmem, hbm, vmem, vmem, vmem, hbm, vmem, hbm, hbm, hbm, vmem, vmem],
        out_specs=vmem,
        scratch_shapes=[
            pltpu.VMEM((NZ, NY, NC, 80, 256), BF16),
            pltpu.VMEM((NZ, NY, NC, 64, 256), BF16),
            pltpu.VMEM((NZ, NY, NC, 32, 1408), BF16),
            pltpu.VMEM((NZ, NY, NC, 32, 1408), BF16),
            pltpu.VMEM((NZ, NY, NC, 32, DOWN_A), BF16),
            pltpu.VMEM((NZ, NY, NC, 32, 1408 - DOWN_A), BF16),
            pltpu.VMEM((4, 256, 2048), BF16),
            pltpu.VMEM((4, 256, 256), BF16),
            pltpu.VMEM((4, 256, 128), BF16),
            pltpu.VMEM((4, 256, 128), F32),
            pltpu.VMEM((4, 256, 128), F32),
            pltpu.VMEM((4, 256, 64), F32),
            pltpu.VMEM((2, 256, 1024), F32),
            pltpu.VMEM((2, 256, 1024), BF16),
            pltpu.VMEM((256, 2048), BF16),
            pltpu.VMEM((4, 64, 2048), F32),
            pltpu.VMEM((8, 256, 256), BF16),
            pltpu.VMEM((256, 1408), BF16),
            pltpu.VMEM((8, 4, 64, 256), BF16),
            pltpu.VMEM((8, 3, 64, 256), BF16),
            dma((6, 31)),
            dma((6, 2)),
            dma((6, 8)),
            dma((6, 8)),
            dma((3,)),
            dma((3,)),
            dma((3,)),
            dma((3,)),
            dma((3,)),
            dma((3,)),
            dma((8, 3)),
            dma((8, 3)),
            dma((8, 3)),
            dma((8, 3)),
            dma((7,)),
        ],
        compiler_params=pltpu.CompilerParams(
            collective_id=0, has_side_effects=True, vmem_limit_bytes=60 * 1024 * 1024
        ),
    )(
        tokens_in,
        queries,
        keys.T,
        values.T,
        doc_ids.reshape(1, -1),
        query_gain.reshape(1, -1),
        key_norm_scale.reshape(1, -1),
        out_weight,
        norm_gain.reshape(1, -1),
        gate_weight,
        up_weight,
        down_weight.T,
        jnp.asarray(row),
        jnp.asarray(col),
    )
    return out.reshape(256, 2048)


def solution(mesh):
    return jax.shard_map(
        per_device,
        mesh=mesh,
        in_specs=(
            P("sp", None),
            P("sp", "tp"),
            P("sp", "tp"),
            P("sp", "tp"),
            P("sp"),
            P(),
            P(),
            P("tp", None),
            P(),
            P("sp", "tp"),
            P("sp", "tp"),
            P("tp", "sp"),
        ),
        out_specs=P("sp", None),
        check_vma=False,
    )
```

```python
import heapq
import jax
import jax.numpy as jnp
import numpy as np
from jax import lax
from jax.experimental import pallas as pl
from jax.experimental.pallas import tpu as pltpu
from jax.sharding import PartitionSpec as P

GRID = 64
EPS = 1e-06
THETA = 10000.0
NEG = -1e30
NZ, NY, NC, NX = 8, 4, 2, 4
DZS = (0, 1, -1, 2, -2, 3, -3, 4)
DYS = (0, 1, -1, 2)
MESH = pl.DeviceIdType.MESH
F32, BF16 = jnp.float32, jnp.bfloat16

DOWN_A = 768
PARTS = (
    ("k", "zy", 0, 0.88, 19.3),
    ("v", "yz", 1, 0.70, 3.1),
    ("g", "zy", 1, 1.93, 44.4),
    ("u", "yz", 0, 1.93, 57.4),
    ("a", "zy", 0, 1.93 * 6 / 11, 74.5),
    ("b", "yz", 1, 1.93 * 5 / 11, 91.7),
)
HOP = 4.9
BACKLOG = 2.0
LATENCY = 2.9


def spread(order, flip):
    messages = {}

    def z_ring(dy, up):
        for d in (1, 2, 3):
            messages[-d, dy] = ("z+", (-d + 1, dy))
            messages[d, dy] = ("z-", (d - 1, dy))
        messages[4, dy] = ("z+", (-3, dy)) if up else ("z-", (3, dy))

    def y_ring(dz, up):
        messages[dz, -1] = ("y+", (dz, 0))
        messages[dz, 1] = ("y-", (dz, 0))
        messages[dz, 2] = ("y+", (dz, -1)) if up else ("y-", (dz, 1))

    if order == "zy":
        z_ring(0, flip)
        for n, dz in enumerate(sorted(DZS)):
            y_ring(dz, (n + flip) % 2 == 0)
    else:
        y_ring(0, flip)
        for n, dy in enumerate(sorted(DYS)):
            z_ring(dy, (n + flip) % 2 == 0)
    return messages


def plan():
    received = {p[0]: spread(p[1], p[2]) for p in PARTS}
    cost = {p[0]: p[3] for p in PARTS}
    due = {p[0]: p[4] for p in PARTS}
    times = {"first": 2.1, "attend": 2.1, "half": 1.15, "pair": 0.25, "attended": 1.2, "mix": 0.7, "norm": 0.6, "gateup": 0.78, "down": 0.4, "reduce": 0.2}
    follow = {}
    for part, messages in received.items():
        for key, (link, held) in messages.items():
            follow.setdefault((part, held), []).append((link, key))

    def depth(part, key):
        return max([1 + depth(part, k) for _, k in follow.get((part, key), [])], default=0)

    now, count, order = 0.0, 0, []
    link_free = {link: 0.0 for link in ("z+", "z-", "y+", "y-", "d", "x")}
    queues = {link: [] for link in ("z+", "z-", "y+", "y-")}
    arrivals = []
    have, sib, done = set(), set(), set()

    def push(when, *event):
        nonlocal count
        count += 1
        heapq.heappush(arrivals, (when, count) + event)

    def got(part, key):
        nonlocal count
        have.add((part, key))
        for link, k in follow.get((part, key), []):
            count += 1
            heapq.heappush(queues[link], (due[part] - depth(part, k) * (cost[part] + HOP), count, part, k, key))
        dz = key[0]
        if part in "kv" and dz == 0:
            order.append(("one", part, key[1]))
            link_free["d"] = max(now, link_free["d"]) + 0.1
            push(link_free["d"] + 1.7, "one", part, key[1])
        elif all((part, (dz, dy)) in have for dy in DYS):
            order.append(("sib", part, dz))
            start = max(now, link_free["d"])
            link_free["d"] = start + 0.3
            push(start + 2.0, "sib", part, dz)

    def tick():
        while arrivals and arrivals[0][0] <= now:
            _, _, kind, part, key = heapq.heappop(arrivals)
            order.append(("wait" + kind, part, key))
            if kind == "sib":
                sib.add((part, key))
            elif kind == "":
                got(part, key)
            elif kind == "one":
                done.add((kind, part, key))
            else:
                done.add((kind, part))
        for link, queue in queues.items():
            while queue and link_free[link] - now < BACKLOG:
                _, _, part, key, held = heapq.heappop(queue)
                order.append(("send", part, key, held, link))
                link_free[link] = max(now, link_free[link]) + cost[part]
                push(link_free[link] + LATENCY, "", part, key)

    def near(parts, dz):
        return all((p, (dz, dy)) in have for p in parts for dy in DYS)

    def ready(step):
        kind = step[0]
        if kind == "first":
            return near("kv", 0) and all(("one", p, dy) in done for p in "kv" for dy in step[1:])
        if kind in ("attend", "half"):
            return near("kv", step[1]) if step[2] else all((p, step[1]) in sib for p in "kv")
        if kind == "gateup":
            return all(near("gu", dz) and all((p, dz) in sib for p in "gu") for dz in DZS)
        if kind == "mix":
            return ("att", step[1]) in done
        if kind == "down":
            return near("ab", step[1]) and all((p, step[1]) in sib for p in "ab")
        if kind == "reduce":
            return ("rs", step[1]) in done
        return True

    def run(step):
        nonlocal now
        order.append(step)
        now += times[step[0]]
        if step[0] == "pair":
            link_free["x"] = now + 2.8
        if step[0] == "attended":
            for n, length in enumerate((1.4, 1.5, 2.8)):
                push(max(now - 0.8, link_free["x"]) + length + LATENCY, "att", n, 0)
        if step[0] == "down":
            link_free["x"] = max(now, link_free["x"]) + 1.4
            push(link_free["x"] + LATENCY, "rs", step[1], 0)

    def advance():
        nonlocal now
        now = max(now, arrivals[0][0])
        tick()

    for part in "kvgu":
        got(part, (0, 0))
    tick()
    order.append(("more",))
    for part in "ab":
        got(part, (0, 0))
    now = 0.75
    steps = [("first", 0, 1), ("first", -1, 2), ("attend", DZS[1], True)]
    for n in range(1, 7):
        steps += [("attend", DZS[n + 1], True), ("attend", DZS[n], False)]
    steps.append(("attend", DZS[7], False))
    halves = [("half", *step[1:]) for step in steps[12:]]
    steps = steps[:12] + halves + [("pair", 0)] + halves + [("attended", 0)]
    steps += [("mix", 0), ("mix", 1), ("mix", 2), ("norm", 0)]
    steps += [("gateup", n) for n in range(6)]
    for step in steps:
        tick()
        while not ready(step):
            advance()
        run(step)
    downs, reduces = list(DZS), []
    while downs or reduces:
        tick()
        steps = [("reduce", dz) for dz in reduces] + [("down", dz) for dz in downs]
        step = next((step for step in steps if ready(step)), None)
        if step is None:
            advance()
            continue
        run(step)
        if step[0] == "down":
            downs.remove(step[1])
            reduces.append(step[1])
        else:
            reduces.remove(step[1])
    while arrivals:
        advance()
    order.append(("end",))
    return order, now


def turn_tables():
    lane = np.arange(64)
    freqs = THETA ** (-2.0 * (lane % 16) / 32.0)
    sign = np.where(lane % 32 < 16, -1.0, 1.0)
    rows = np.arange(256)[:, None] * freqs[None]
    by_row = lane < 32
    row_cos = np.where(by_row, np.cos(rows), 0.0).reshape(64, 4, 64)
    row_sin = np.where(by_row, np.sin(rows) * sign, 0.0).reshape(64, 4, 64)
    row = np.concatenate([row_cos, row_sin], axis=1)
    cols = np.arange(64)[:, None] * freqs[None]
    col_cos = np.where(by_row, 0.0, np.cos(cols))
    col_sin = np.where(by_row, 0.0, np.sin(cols) * sign)
    col = np.stack([col_cos, col_sin])
    return np.tile(row, (1, 1, 2)).astype(np.float32), np.tile(col, (1, 1, 2)).astype(np.float32)


def nt(a, b):
    return lax.dot_general(a, b, (((1,), (1,)), ((), ())), preferred_element_type=F32)


def nn(a, b):
    return lax.dot_general(a, b, (((1,), (0,)), ((), ())), preferred_element_type=F32)


def kernel(
    tokens_ref,
    q_ref,
    k_ref,
    v_ref,
    doc_ref,
    qg_ref,
    kg_ref,
    ow_ref,
    ng_ref,
    gate_ref,
    up_ref,
    down_ref,
    row_ref,
    col_ref,
    out_ref,
    kt,
    vt,
    wg,
    wu,
    wa,
    wb,
    ow,
    att,
    qs,
    m_ref,
    l_ref,
    acc_ref,
    s_ref,
    p_ref,
    tok,
    resid,
    normed,
    hidden,
    part_buf,
    rs_buf,
    mine,
    recv_sem,
    send_sem,
    sib_recv,
    sib_send,
    ow_recv,
    ow_send,
    ow_sib_recv,
    ow_sib_send,
    att_recv,
    att_send,
    rs_recv,
    rs_send,
    ag_recv,
    ag_send,
    local_sem,
    drain_sem,
    one_recv,
):
    s = lax.axis_index("sp")
    x = lax.axis_index("tp")
    c = lax.rem(s, NC)
    y = lax.rem(s // NC, NY)
    z = s // (NC * NY)

    z_at = {dz: lax.rem(z + (dz + NZ), NZ) for dz in DZS}
    y_at = {dy: lax.rem(y + (dy + NY), NY) for dy in DYS}
    x_at = {dx: lax.rem(x + (dx + NX), NX) for dx in DYS}
    wz, wy, wx = z_at.__getitem__, y_at.__getitem__, x_at.__getitem__

    def at(zz, yy, cc, xx):
        return ((zz * NY + yy) * NC + cc, xx)

    neighbour = {
        "z+": at(wz(1), y, c, x),
        "z-": at(wz(-1), y, c, x),
        "y+": at(z, wy(1), c, x),
        "y-": at(z, wy(-1), c, x),
    }
    sibling = at(z, y, 1 - c, x)
    x_plus = at(z, y, c, wx(1))
    x_minus = at(z, y, c, wx(-1))
    x_far = at(z, y, c, wx(2))

    arrays = {"k": kt, "v": vt, "g": wg, "u": wu, "a": wa, "b": wb}
    names = [p[0] for p in PARTS]
    received = {p[0]: spread(p[1], p[2]) for p in PARTS}
    index = {name: {key: n for n, key in enumerate(received[name])} for name in names}

    local = [
        pltpu.make_async_copy(v_ref, vt.at[z, y, c], local_sem.at[0]),
        pltpu.make_async_copy(gate_ref, wg.at[z, y, c], local_sem.at[1]),
        pltpu.make_async_copy(up_ref, wu.at[z, y, c], local_sem.at[2]),
        pltpu.make_async_copy(down_ref.at[:, :DOWN_A], wa.at[z, y, c], local_sem.at[3]),
        pltpu.make_async_copy(down_ref.at[:, DOWN_A:], wb.at[z, y, c], local_sem.at[4]),
        pltpu.make_async_copy(ow_ref, ow.at[x], local_sem.at[5]),
        pltpu.make_async_copy(tokens_ref, tok, local_sem.at[6]),
    ]
    for copy in local:
        copy.start()

    barrier = pltpu.get_barrier_semaphore()
    for who in (*neighbour.values(), sibling, x_plus, x_minus, x_far):
        pl.semaphore_signal(barrier, inc=1, device_id=who, device_id_type=MESH)

    lane = lax.broadcasted_iota(jnp.int32, (256, 128), 1)
    low = lane < 64
    swap_up = lax.rem(lane // 16, 2) == 0
    row = row_ref[s]
    cos = jnp.concatenate([jnp.broadcast_to(row[r : r + 1], (64, 128)) + col_ref[0] for r in range(4)], axis=0)
    sin = jnp.concatenate([jnp.broadcast_to(row[r + 4 : r + 5], (64, 128)) + col_ref[1] for r in range(4)], axis=0)

    def turned(values, gain):
        square = values * values
        lo = jnp.sum(jnp.where(low, square, 0.0), axis=1, keepdims=True)
        hi = jnp.sum(jnp.where(low, 0.0, square), axis=1, keepdims=True)
        mean = jnp.where(low, lo, hi) * (1.0 / 64.0)
        values = values * lax.rsqrt(mean + EPS) * gain
        other = jnp.where(swap_up, pltpu.roll(values, 112, 1), pltpu.roll(values, 16, 1))
        return values * cos + other * sin

    def eye(n):
        return (
            lax.broadcasted_iota(jnp.int32, (n, n), 0) == lax.broadcasted_iota(jnp.int32, (n, n), 1)
        ).astype(F32).astype(BF16)

    keys = k_ref[...].astype(F32)
    gain = jnp.where(
        lax.broadcasted_iota(jnp.int32, (64, 64), 0) == lax.broadcasted_iota(jnp.int32, (64, 64), 1), kg_ref[...], 0.0
    )
    keys = keys * lax.rsqrt(jnp.mean(keys * keys, axis=0, keepdims=True) + EPS) * jnp.sum(gain, axis=1, keepdims=True)
    other = jnp.concatenate([keys[16:32], keys[0:16], keys[48:64], keys[32:48]], axis=0)
    keys = keys * jnp.transpose(cos)[:64] + other * jnp.transpose(sin)[:64]
    docs = jnp.broadcast_to(doc_ref[...], (16, 256))
    same = lax.broadcasted_iota(jnp.int32, (16, 256), 0) == docs
    kt[z, y, c, 0:64, :] = keys.astype(BF16)
    kt[z, y, c, 64:80, :] = jnp.where(same, NEG, 0.0).astype(BF16)
    local[0].wait()

    pl.semaphore_wait(barrier, 8)

    def send(part, key, held, link):
        n = index[part][key]
        ref = arrays[part]
        slot = ref.at[wz(held[0]), wy(held[1]), c]
        i = names.index(part)
        which = 0 if n < 28 else 1
        return pltpu.make_async_remote_copy(
            src_ref=slot,
            dst_ref=slot,
            send_sem=send_sem.at[i, which],
            recv_sem=recv_sem.at[i, n],
            device_id=neighbour[link],
            device_id_type=MESH,
        )

    def wait_recv(part, key):
        n = index[part][key]
        i = names.index(part)
        slot = arrays[part].at[wz(key[0]), wy(key[1]), c]
        pltpu.make_async_remote_copy(
            src_ref=slot,
            dst_ref=slot,
            send_sem=send_sem.at[i, 0],
            recv_sem=recv_sem.at[i, n],
            device_id=sibling,
            device_id_type=MESH,
        ).wait_recv()

    def to_sibling(part, dz, cc):
        i = names.index(part)
        slots = arrays[part].at[wz(dz), :, cc]
        return pltpu.make_async_remote_copy(
            src_ref=slots,
            dst_ref=slots,
            send_sem=sib_send.at[i],
            recv_sem=sib_recv.at[i, DZS.index(dz)],
            device_id=sibling,
            device_id_type=MESH,
        )

    def one_to_sibling(part, dy, cc):
        i = names.index(part)
        slot = arrays[part].at[z, wy(dy), cc]
        return pltpu.make_async_remote_copy(
            src_ref=slot,
            dst_ref=slot,
            send_sem=sib_send.at[i],
            recv_sem=one_recv.at[i, DYS.index(dy)],
            device_id=sibling,
            device_id_type=MESH,
        )

    def together(ref, send=None, recv=None):
        copy = pltpu.make_async_remote_copy(
            src_ref=ref,
            dst_ref=ref,
            send_sem=drain_sem.at[0] if send is None else send,
            recv_sem=drain_sem.at[0] if recv is None else recv,
            device_id=sibling,
            device_id_type=MESH,
        )
        copy.wait_send() if send is not None else copy.wait_recv()

    def half(member):
        return ow.at[member, pl.ds(pl.multiple_of(128 * c, 128), 128)]

    def ow_copy(member, n, who):
        return pltpu.make_async_remote_copy(
            src_ref=half(member),
            dst_ref=half(member),
            send_sem=ow_send.at[0],
            recv_sem=ow_recv.at[0],
            device_id=who,
            device_id_type=MESH,
        )

    def other_half(member, mine):
        cc = c if mine else 1 - c
        return ow.at[member, pl.ds(pl.multiple_of(128 * cc, 128), 128)]

    def ow_sib(member, n, mine):
        ref = other_half(member, mine)
        return pltpu.make_async_remote_copy(
            src_ref=ref,
            dst_ref=ref,
            send_sem=ow_sib_send.at[0],
            recv_sem=ow_sib_recv.at[0],
            device_id=sibling,
            device_id_type=MESH,
        )

    def att_copy(member, pair, n, who):
        return pltpu.make_async_remote_copy(
            src_ref=att.at[member, pair],
            dst_ref=att.at[member, pair],
            send_sem=att_send.at[0],
            recv_sem=att_recv.at[n],
            device_id=who,
            device_id_type=MESH,
        )

    def rs_copy(j, member, n, who):
        return pltpu.make_async_remote_copy(
            src_ref=part_buf.at[j, member],
            dst_ref=rs_buf.at[j, n],
            send_sem=rs_send.at[0],
            recv_sem=rs_recv.at[j],
            device_id=who,
            device_id_type=MESH,
        )

    def out_chunk(dz):
        return out_ref.at[x, :, pl.ds(pl.multiple_of(256 * wz(dz), 256), 256)]

    def ag_copy(j, who):
        return pltpu.make_async_remote_copy(
            src_ref=mine.at[j],
            dst_ref=out_chunk(DZS[j]),
            send_sem=ag_send.at[0],
            recv_sem=ag_recv.at[0],
            device_id=who,
            device_id_type=MESH,
        )

    def more():
        local[5].wait()
        ow_copy(x, 2, x_far).start()
        ow_copy(x, 0, x_plus).start()
        ow_copy(x, 1, x_minus).start()
        no = jnp.where(same, 0.0, 1.0).astype(BF16)
        no = jnp.concatenate([jnp.zeros((64, 256), BF16), no, jnp.zeros((48, 256), BF16)], axis=0)
        no_t = nt(eye(256), no)
        query_gain = jnp.concatenate([qg_ref[...], qg_ref[...]], axis=1)
        for pair in range(2):
            both = turned(q_ref[:, 128 * pair : 128 * pair + 128].astype(F32), query_gain) * 0.125
            for odd in range(2):
                head = pltpu.roll(both, 64, 1) if odd else both
                qs[2 * pair + odd] = jnp.where(low, head, no_t).astype(BF16)
        m_ref[...] = jnp.full((4, 256, 128), NEG, F32)
        l_ref[...] = jnp.zeros((4, 256, 128), F32)
        acc_ref[...] = jnp.zeros((4, 256, 64), F32)
        local[3].wait()
        local[4].wait()

    def ow_forward():
        together(ow.at[0:3, 0:128], recv=ow_recv.at[0])
        for n, member in enumerate((wx(-1), wx(1), wx(2))):
            ow_sib(member, n, True).start()

    def ow_wait():
        together(ow.at[0:3, 0:128], recv=ow_sib_recv.at[0])

    def attend(i, heads):
        e0, e1, e2, e15 = (1 // (1 + (i - k) * (i - k)) for k in (0, 1, 2, 15))
        odd, start = lax.rem(i, 2), e0 + e1
        far = odd * ((i + 1) // 2) + (1 - odd) * (i // 2 - 1) + e0 - e1 + e2 - e15
        zz = lax.rem(z + NZ + (far + 1) // 2 * (2 * lax.rem(far, 2) - 1), NZ)
        cc = lax.rem(c + 1 - odd - e2 + e15, 2)
        pieces = [
            (
                start * lax.rem(y + 2 * i + j // 2, NY) + (1 - start) * j,
                start * (j % 2) + (1 - start) * cc,
            )
            for j in range(4)
        ]

        def scores(n):
            q = qs[heads[n]][:, :80]
            for j in range(4):
                s_ref[n % 2, :, 256 * j : 256 * j + 256] = nn(q, kt[zz, pieces[j][0], pieces[j][1]])

        scores(0)
        for n, h in enumerate(heads):
            if n + 1 < len(heads):
                scores(n + 1)
            for r in range(0, 256, 32):
                rows = slice(r, r + 32)
                sc = s_ref[n % 2, rows, :]
                old = m_ref[h, rows, :]
                new = jnp.maximum(old, jnp.max(sc, axis=1, keepdims=True))
                shrink = jnp.exp(old - new)
                m_ref[h, rows, :] = new
                w = jnp.exp(sc - new[:, :1])
                part = w[:, :128]
                for t in range(1, 8):
                    part = part + w[:, 128 * t : 128 * t + 128]
                l_ref[h, rows, :] = l_ref[h, rows, :] * shrink + part
                acc_ref[h, rows, :] = acc_ref[h, rows, :] * shrink[:, :64]
                p_ref[n % 2, rows, :] = w.astype(BF16)
            pv = nt(p_ref[n % 2, :, 0:256], vt[zz, pieces[0][0], pieces[0][1]])
            for j in range(1, 4):
                pv = pv + nt(p_ref[n % 2, :, 256 * j : 256 * j + 256], vt[zz, pieces[j][0], pieces[j][1]])
            acc_ref[h] = acc_ref[h] + pv

    def add(n, member, start):
        rows = slice(128 * n, 128 * n + 128)
        share = nn(att[member, 0, rows, :], ow[member, 0:128, :]) + nn(att[member, 1, rows, :], ow[member, 128:256, :])
        share = share.astype(BF16).astype(F32)
        if start is None:
            start = resid[2 * n : 2 * n + 2].reshape(128, 2048)
        resid[2 * n : 2 * n + 2] = (start + share).reshape(2, 64, 2048)

    def attended(pair):
        pieces = []
        for h in (2 * pair, 2 * pair + 1):
            total = jnp.sum(l_ref[h], axis=1, keepdims=True)
            pieces.append(acc_ref[h] / total)
        att[x, pair] = jnp.concatenate(pieces, axis=1).astype(BF16)
        att_copy(x, pair, 0, x_plus).start()
        att_copy(x, pair, 1, x_minus).start()
        att_copy(x, pair, 2, x_far).start()

    def own_share():
        ow_wait()
        local[6].wait()
        for n in range(2):
            rows = slice(128 * n, 128 * n + 128)
            add(n, x, tok[rows, :].astype(F32))

    def mix(n):
        for half_rows in range(2):
            add(half_rows, wx((-1, 1, 2)[n]), None)

    def norm():
        for n in range(2):
            total = resid[2 * n : 2 * n + 2].reshape(128, 2048)
            mean = jnp.mean(total * total, axis=1, keepdims=True)
            scaled = (total * lax.rsqrt(mean + EPS) * ng_ref[...]).astype(BF16)
            for t in range(8):
                normed[t, 128 * n : 128 * n + 128, :] = scaled[:, 256 * t : 256 * t + 256]

    def gateup(n):
        cols = slice(256 * n, min(256 * n + 256, 1408))
        width = cols.stop - cols.start
        gate = jnp.zeros((256, width), F32)
        up = jnp.zeros((256, width), F32)
        for t in range(8):
            a = normed[t]
            gate = gate + nn(a, wg[t, :, :, :, cols].reshape(256, width))
            up = up + nn(a, wu[t, :, :, :, cols].reshape(256, width))
        hidden[:, cols] = (gate / (1.0 + jnp.exp(-gate)) * up).astype(BF16)

    def down(dz):
        j = DZS.index(dz)
        zz = wz(dz)
        fed = nt(hidden[:, :DOWN_A], wa[zz].reshape(256, DOWN_A))
        fed = (fed + nt(hidden[:, DOWN_A:], wb[zz].reshape(256, 1408 - DOWN_A))).astype(BF16)
        for member in range(4):
            part_buf[j, member] = fed[64 * member : 64 * member + 64]
        rs_copy(j, wx(2), 2, x_far).start()
        rs_copy(j, wx(1), 0, x_plus).start()
        rs_copy(j, wx(-1), 1, x_minus).start()

    def wait_rs(dz):
        j = DZS.index(dz)
        together(rs_buf.at[j], recv=rs_recv.at[j])

    def reduce(dz):
        j = DZS.index(dz)
        total = part_buf[j, x].astype(F32)
        for n in range(3):
            total = total + rs_buf[j, n].astype(F32)
        cols = pl.ds(pl.multiple_of(256 * wz(dz), 256), 256)
        mine[j] = (resid[x, :, cols] + total).astype(BF16)
        ag_copy(j, x_far).start()
        ag_copy(j, x_plus).start()
        ag_copy(j, x_minus).start()
        pltpu.make_async_copy(mine.at[j], out_chunk(dz), drain_sem.at[1]).start()

    def end():
        for i, name in enumerate(names):
            ref = arrays[name]
            many = ref.at[0:7, :, 0]
            few = ref.at[0, 0:3, 0]
            pltpu.make_async_remote_copy(
                src_ref=many,
                dst_ref=many,
                send_sem=send_sem.at[i, 0],
                recv_sem=recv_sem.at[i, 0],
                device_id=sibling,
                device_id_type=MESH,
            ).wait_send()
            pltpu.make_async_remote_copy(
                src_ref=few,
                dst_ref=few,
                send_sem=send_sem.at[i, 1],
                recv_sem=recv_sem.at[i, 0],
                device_id=sibling,
                device_id_type=MESH,
            ).wait_send()
            every = ref.at[:, :, c]
            pltpu.make_async_remote_copy(
                src_ref=every,
                dst_ref=every,
                send_sem=sib_send.at[i],
                recv_sem=recv_sem.at[i, 0],
                device_id=sibling,
                device_id_type=MESH,
            ).wait_send()
        together(ow.at[0:3, 0:128], send=ow_send.at[0])
        together(ow.at[0:3, 0:128], send=ow_sib_send.at[0])
        together(att.at[0:3], send=att_send.at[0])
        together(part_buf.at[0:6], send=rs_send.at[0])
        together(part_buf.at[0:6], send=ag_send.at[0])
        pltpu.make_async_copy(mine, mine, drain_sem.at[1]).wait()
        together(part_buf.at[0:6], recv=ag_recv.at[0])

    done = set()

    def handle(event):
        kind = event[0]
        if kind == "send":
            _, part, key, held, link = event
            if part in "gu" and part not in done:
                local[1 + "gu".index(part)].wait()
                done.add(part)
            send(part, key, held, link).start()
        elif kind == "wait":
            wait_recv(event[1], event[2])
        elif kind == "sib":
            to_sibling(event[1], event[2], c).start()
        elif kind == "one":
            one_to_sibling(event[1], event[2], c).start()
        elif kind == "waitone":
            one_to_sibling(event[1], event[2], 1 - c).wait_recv()
        elif kind == "waitsib":
            to_sibling(event[1], event[2], 1 - c).wait_recv()
        elif kind == "more":
            more()
        elif kind == "attended":
            attended(1)
            own_share()
        elif kind == "pair":
            attended(0)
        elif kind == "waitatt":
            together(att.at[wx((-1, 1, 2)[event[1]])], recv=att_recv.at[event[1]])
        elif kind == "mix":
            mix(event[1])
        elif kind == "norm":
            norm()
        elif kind == "gateup":
            gateup(event[1])
        elif kind == "down":
            down(event[1])
        elif kind == "waitrs":
            wait_rs(event[1])
        elif kind == "reduce":
            reduce(event[1])
        elif kind == "end":
            end()

    order, _ = plan()
    attends = [n for n, event in enumerate(order) if event[0] in ("first", "attend", "half")]
    attends.append(attends[-1] + 1)
    for event in order[: attends[0]]:
        handle(event)

    def between(i, low, high):
        for n in range(low, high):

            @pl.when(i == n)
            def _():
                for event in order[attends[n] + 1 : attends[n + 1]]:
                    handle(event)
                if n == 11:
                    ow_forward()

    def step(i, carry):
        attend(i, range(4))
        between(i, 0, 12)
        return carry

    def half_step(i, carry):
        pair = (i - 12) // 4
        attend(12 + lax.rem(i, 4), (2 * pair, 2 * pair + 1))
        between(i, 12, 20)
        return carry

    lax.fori_loop(0, 12, step, 0)
    lax.fori_loop(12, 20, half_step, 0)
    for event in order[attends[-1] :]:
        handle(event)


def per_device(
    tokens_in,
    queries,
    keys,
    values,
    doc_ids,
    query_gain,
    key_norm_scale,
    out_weight,
    norm_gain,
    gate_weight,
    up_weight,
    down_weight,
):
    row, col = turn_tables()
    vmem = pl.BlockSpec(memory_space=pltpu.VMEM)
    anywhere = pl.BlockSpec(memory_space=pl.ANY)
    hbm = pl.BlockSpec(memory_space=pltpu.HBM)
    dma = pltpu.SemaphoreType.DMA
    out = pl.pallas_call(
        kernel,
        name="layer",
        out_shape=jax.ShapeDtypeStruct((4, 64, 2048), BF16),
        in_specs=[hbm, vmem, vmem, hbm, vmem, vmem, vmem, hbm, vmem, hbm, hbm, hbm, vmem, vmem],
        out_specs=anywhere,
        scratch_shapes=[
            pltpu.VMEM((NZ, NY, NC, 80, 256), BF16),
            pltpu.VMEM((NZ, NY, NC, 64, 256), BF16),
            pltpu.VMEM((NZ, NY, NC, 32, 1408), BF16),
            pltpu.VMEM((NZ, NY, NC, 32, 1408), BF16),
            pltpu.VMEM((NZ, NY, NC, 32, DOWN_A), BF16),
            pltpu.VMEM((NZ, NY, NC, 32, 1408 - DOWN_A), BF16),
            pltpu.VMEM((4, 256, 2048), BF16),
            pltpu.VMEM((4, 2, 256, 128), BF16),
            pltpu.VMEM((4, 256, 128), BF16),
            pltpu.VMEM((4, 256, 128), F32),
            pltpu.VMEM((4, 256, 128), F32),
            pltpu.VMEM((4, 256, 64), F32),
            pltpu.VMEM((2, 256, 1024), F32),
            pltpu.VMEM((2, 256, 1024), BF16),
            pltpu.VMEM((256, 2048), BF16),
            pltpu.VMEM((4, 64, 2048), F32),
            pltpu.VMEM((8, 256, 256), BF16),
            pltpu.VMEM((256, 1408), BF16),
            pltpu.VMEM((8, 4, 64, 256), BF16),
            pltpu.VMEM((8, 3, 64, 256), BF16),
            pltpu.VMEM((8, 64, 256), BF16),
            dma((6, 31)),
            dma((6, 2)),
            dma((6, 8)),
            dma((6,)),
            dma((1,)),
            dma((1,)),
            dma((1,)),
            dma((1,)),
            dma((3,)),
            dma((1,)),
            dma((8,)),
            dma((1,)),
            dma((1,)),
            dma((1,)),
            dma((7,)),
            dma((2,)),
            dma((2, 4)),
        ],
        compiler_params=pltpu.CompilerParams(
            collective_id=0, has_side_effects=True, vmem_limit_bytes=60 * 1024 * 1024
        ),
    )(
        tokens_in,
        queries,
        keys.T,
        values.T,
        doc_ids.reshape(1, -1),
        query_gain.reshape(1, -1),
        key_norm_scale.reshape(1, -1),
        out_weight,
        norm_gain.reshape(1, -1),
        gate_weight,
        up_weight,
        down_weight.T,
        jnp.asarray(row),
        jnp.asarray(col),
    )
    return out.reshape(256, 2048)


def solution(mesh):
    return jax.shard_map(
        per_device,
        mesh=mesh,
        in_specs=(
            P("sp", None),
            P("sp", "tp"),
            P("sp", "tp"),
            P("sp", "tp"),
            P("sp"),
            P(),
            P(),
            P("tp", None),
            P(),
            P("sp", "tp"),
            P("sp", "tp"),
            P("tp", "sp"),
        ),
        out_specs=P("sp", None),
        check_vma=False,
    )
```

```python
import heapq
import jax
import jax.numpy as jnp
import numpy as np
from jax import lax
from jax.experimental import pallas as pl
from jax.experimental.pallas import tpu as pltpu
from jax.sharding import PartitionSpec as P

GRID = 64
EPS = 1e-06
THETA = 10000.0
NEG = -1e30
NZ, NY, NC, NX = 8, 4, 2, 4
DZS = (0, 1, -1, 2, -2, 3, -3, 4)
DYS = (0, 1, -1, 2)
MESH = pl.DeviceIdType.MESH
F32, BF16 = jnp.float32, jnp.bfloat16

DOWN_A = 1024
PARTS = (
    ("k", "zy", 0, 0.88, 15.8),
    ("v", "yz", 1, 0.70, 8.6),
    ("g", "zy", 1, 1.93, 30.8),
    ("u", "yz", 1, 1.93, 32.7),
    ("a", "zy", 0, 1.93 * 8 / 11, 47.5),
    ("b", "yz", 1, 1.93 * 3 / 11, 57.9),
)
HOP = 3.7
BACKLOG = 2.0
LATENCY = 2.9


def spread(order, flip):
    messages = {}

    def z_ring(dy, up):
        for d in (1, 2, 3):
            messages[-d, dy] = ("z+", (-d + 1, dy))
            messages[d, dy] = ("z-", (d - 1, dy))
        messages[4, dy] = ("z+", (-3, dy)) if up else ("z-", (3, dy))

    def y_ring(dz, up):
        messages[dz, -1] = ("y+", (dz, 0))
        messages[dz, 1] = ("y-", (dz, 0))
        messages[dz, 2] = ("y+", (dz, -1)) if up else ("y-", (dz, 1))

    if order == "zy":
        z_ring(0, flip)
        for n, dz in enumerate(sorted(DZS)):
            y_ring(dz, (n + flip) % 2 == 0)
    else:
        y_ring(0, flip)
        for n, dy in enumerate(sorted(DYS)):
            z_ring(dy, (n + flip) % 2 == 0)
    return messages


def plan():
    received = {p[0]: spread(p[1], p[2]) for p in PARTS}
    cost = {p[0]: p[3] for p in PARTS}
    due = {p[0]: p[4] for p in PARTS}
    times = {"first": 2.1, "attend": 2.1, "attended": 1.2, "mix": 0.7, "norm": 0.6, "gateup": 0.78, "down": 0.4, "reduce": 0.2}
    follow = {}
    for part, messages in received.items():
        for key, (link, held) in messages.items():
            follow.setdefault((part, held), []).append((link, key))

    def depth(part, key):
        return max([1 + depth(part, k) for _, k in follow.get((part, key), [])], default=0)

    now, count, order = 0.0, 0, []
    link_free = {link: 0.0 for link in ("z+", "z-", "y+", "y-", "d", "x")}
    queues = {link: [] for link in ("z+", "z-", "y+", "y-")}
    arrivals = []
    have, sib, done = set(), set(), set()

    def push(when, *event):
        nonlocal count
        count += 1
        heapq.heappush(arrivals, (when, count) + event)

    def got(part, key):
        nonlocal count
        have.add((part, key))
        for link, k in follow.get((part, key), []):
            count += 1
            heapq.heappush(queues[link], (due[part] - depth(part, k) * (cost[part] + HOP), count, part, k, key))
        dz = key[0]
        if part in "kv" and dz == 0:
            order.append(("one", part, key[1]))
            link_free["d"] = max(now, link_free["d"]) + 0.1
            push(link_free["d"] + 1.7, "one", part, key[1])
        elif all((part, (dz, dy)) in have for dy in DYS):
            order.append(("sib", part, dz))
            start = max(now, link_free["d"])
            link_free["d"] = start + 0.3
            push(start + 2.0, "sib", part, dz)

    def tick():
        while arrivals and arrivals[0][0] <= now:
            _, _, kind, part, key = heapq.heappop(arrivals)
            order.append(("wait" + kind, part, key))
            if kind == "sib":
                sib.add((part, key))
            elif kind == "":
                got(part, key)
            elif kind == "one":
                done.add((kind, part, key))
            else:
                done.add((kind, part))
        for link, queue in queues.items():
            while queue and link_free[link] - now < BACKLOG:
                _, _, part, key, held = heapq.heappop(queue)
                order.append(("send", part, key, held, link))
                link_free[link] = max(now, link_free[link]) + cost[part]
                push(link_free[link] + LATENCY, "", part, key)

    def near(parts, dz):
        return all((p, (dz, dy)) in have for p in parts for dy in DYS)

    def ready(step):
        kind = step[0]
        if kind == "first":
            return all((p, (0, dy)) in have and ("one", p, dy) in done for p in "kv" for dy in step[1:])
        if kind == "attend":
            return near("kv", step[1]) if step[2] else all((p, step[1]) in sib for p in "kv")
        if kind == "gateup":
            return all(near("gu", dz) and all((p, dz) in sib for p in "gu") for dz in DZS)
        if kind == "mix":
            return ("att", step[1]) in done
        if kind == "down":
            return near("ab", step[1]) and all((p, step[1]) in sib for p in "ab")
        if kind == "reduce":
            return ("rs", step[1]) in done
        return True

    def run(step):
        nonlocal now
        order.append(step)
        now += times[step[0]]
        if step[0] == "attended":
            for n, length in enumerate((2.8, 2.9, 5.5)):
                push(now + length + LATENCY, "att", n, 0)
        if step[0] == "down":
            link_free["x"] = max(now, link_free["x"]) + 1.4
            push(link_free["x"] + LATENCY, "rs", step[1], 0)

    def advance():
        nonlocal now
        now = max(now, arrivals[0][0])
        tick()

    for part in "kvgu":
        got(part, (0, 0))
    tick()
    order.append(("more",))
    for part in "ab":
        got(part, (0, 0))
    now = 0.75
    steps = [("first", 0, 1), ("first", -1, 2), ("attend", DZS[1], True)]
    for n in range(1, 7):
        steps += [("attend", DZS[n + 1], True), ("attend", DZS[n], False)]
    steps += [("attend", DZS[7], False), ("attended", 0), ("mix", 0), ("mix", 1), ("mix", 2), ("norm", 0)]
    steps += [("gateup", n) for n in range(6)]
    for step in steps:
        tick()
        while not ready(step):
            advance()
        run(step)
    downs, reduces = list(DZS), []
    while downs or reduces:
        tick()
        steps = [("reduce", dz) for dz in reduces] + [("down", dz) for dz in downs]
        step = next((step for step in steps if ready(step)), None)
        if step is None:
            advance()
            continue
        run(step)
        if step[0] == "down":
            downs.remove(step[1])
            reduces.append(step[1])
        else:
            reduces.remove(step[1])
    while arrivals:
        advance()
    order.append(("end",))
    return order, now


def turn_tables():
    lane = np.arange(64)
    freqs = THETA ** (-2.0 * (lane % 16) / 32.0)
    sign = np.where(lane % 32 < 16, -1.0, 1.0)
    rows = np.arange(256)[:, None] * freqs[None]
    by_row = lane < 32
    row_cos = np.where(by_row, np.cos(rows), 0.0).reshape(64, 4, 64)
    row_sin = np.where(by_row, np.sin(rows) * sign, 0.0).reshape(64, 4, 64)
    row = np.concatenate([row_cos, row_sin], axis=1)
    cols = np.arange(64)[:, None] * freqs[None]
    col_cos = np.where(by_row, 0.0, np.cos(cols))
    col_sin = np.where(by_row, 0.0, np.sin(cols) * sign)
    col = np.stack([col_cos, col_sin])
    return np.tile(row, (1, 1, 2)).astype(np.float32), np.tile(col, (1, 1, 2)).astype(np.float32)


def nt(a, b):
    return lax.dot_general(a, b, (((1,), (1,)), ((), ())), preferred_element_type=F32)


def nn(a, b):
    return lax.dot_general(a, b, (((1,), (0,)), ((), ())), preferred_element_type=F32)


def kernel(
    tokens_ref,
    q_ref,
    k_ref,
    v_ref,
    doc_ref,
    qg_ref,
    kg_ref,
    ow_ref,
    ng_ref,
    gate_ref,
    up_ref,
    down_ref,
    row_ref,
    col_ref,
    out_ref,
    kt,
    vt,
    wg,
    wu,
    wa,
    wb,
    ow,
    att,
    qs,
    m_ref,
    l_ref,
    acc_ref,
    s_ref,
    p_ref,
    tok,
    resid,
    normed,
    hidden,
    part_buf,
    rs_buf,
    mine,
    recv_sem,
    send_sem,
    sib_recv,
    sib_send,
    ow_recv,
    ow_send,
    ow_sib_recv,
    ow_sib_send,
    att_recv,
    att_send,
    rs_recv,
    rs_send,
    ag_recv,
    ag_send,
    local_sem,
    drain_sem,
    one_recv,
):
    s = lax.axis_index("sp")
    x = lax.axis_index("tp")
    c = lax.rem(s, NC)
    y = lax.rem(s // NC, NY)
    z = s // (NC * NY)

    z_at = {dz: lax.rem(z + (dz + NZ), NZ) for dz in DZS}
    y_at = {dy: lax.rem(y + (dy + NY), NY) for dy in DYS}
    x_at = {dx: lax.rem(x + (dx + NX), NX) for dx in DYS}
    wz, wy, wx = z_at.__getitem__, y_at.__getitem__, x_at.__getitem__

    def at(zz, yy, cc, xx):
        return ((zz * NY + yy) * NC + cc, xx)

    neighbour = {
        "z+": at(wz(1), y, c, x),
        "z-": at(wz(-1), y, c, x),
        "y+": at(z, wy(1), c, x),
        "y-": at(z, wy(-1), c, x),
    }
    sibling = at(z, y, 1 - c, x)
    x_plus = at(z, y, c, wx(1))
    x_minus = at(z, y, c, wx(-1))
    x_far = at(z, y, c, wx(2))

    arrays = {"k": kt, "v": vt, "g": wg, "u": wu, "a": wa, "b": wb}
    names = [p[0] for p in PARTS]
    received = {p[0]: spread(p[1], p[2]) for p in PARTS}
    index = {name: {key: n for n, key in enumerate(received[name])} for name in names}

    local = [
        pltpu.make_async_copy(v_ref, vt.at[z, y, c], local_sem.at[0]),
        pltpu.make_async_copy(gate_ref, wg.at[z, y, c], local_sem.at[1]),
        pltpu.make_async_copy(up_ref, wu.at[z, y, c], local_sem.at[2]),
        pltpu.make_async_copy(down_ref.at[:, :DOWN_A], wa.at[z, y, c], local_sem.at[3]),
        pltpu.make_async_copy(down_ref.at[:, DOWN_A:], wb.at[z, y, c], local_sem.at[4]),
        pltpu.make_async_copy(ow_ref, ow.at[x], local_sem.at[5]),
        pltpu.make_async_copy(tokens_ref, tok, local_sem.at[6]),
    ]
    for copy in local:
        copy.start()

    barrier = pltpu.get_barrier_semaphore()
    for who in (*neighbour.values(), sibling, x_plus, x_minus, x_far):
        pl.semaphore_signal(barrier, inc=1, device_id=who, device_id_type=MESH)

    lane = lax.broadcasted_iota(jnp.int32, (256, 128), 1)
    low = lane < 64
    swap_up = lax.rem(lane // 16, 2) == 0
    row = row_ref[s]
    cos = jnp.concatenate([jnp.broadcast_to(row[r : r + 1], (64, 128)) + col_ref[0] for r in range(4)], axis=0)
    sin = jnp.concatenate([jnp.broadcast_to(row[r + 4 : r + 5], (64, 128)) + col_ref[1] for r in range(4)], axis=0)

    def turned(values, gain):
        square = values * values
        lo = jnp.sum(jnp.where(low, square, 0.0), axis=1, keepdims=True)
        hi = jnp.sum(jnp.where(low, 0.0, square), axis=1, keepdims=True)
        mean = jnp.where(low, lo, hi) * (1.0 / 64.0)
        values = values * lax.rsqrt(mean + EPS) * gain
        other = jnp.where(swap_up, pltpu.roll(values, 112, 1), pltpu.roll(values, 16, 1))
        return values * cos + other * sin

    def eye(n):
        return (
            lax.broadcasted_iota(jnp.int32, (n, n), 0) == lax.broadcasted_iota(jnp.int32, (n, n), 1)
        ).astype(F32).astype(BF16)

    keys = k_ref[...].astype(F32)
    gain = jnp.where(
        lax.broadcasted_iota(jnp.int32, (64, 64), 0) == lax.broadcasted_iota(jnp.int32, (64, 64), 1), kg_ref[...], 0.0
    )
    keys = keys * lax.rsqrt(jnp.mean(keys * keys, axis=0, keepdims=True) + EPS) * jnp.sum(gain, axis=1, keepdims=True)
    other = jnp.concatenate([keys[16:32], keys[0:16], keys[48:64], keys[32:48]], axis=0)
    keys = keys * jnp.transpose(cos)[:64] + other * jnp.transpose(sin)[:64]
    docs = jnp.broadcast_to(doc_ref[...], (16, 256))
    same = lax.broadcasted_iota(jnp.int32, (16, 256), 0) == docs
    kt[z, y, c, 0:64, :] = keys.astype(BF16)
    kt[z, y, c, 64:80, :] = jnp.where(same, NEG, 0.0).astype(BF16)
    local[0].wait()

    pl.semaphore_wait(barrier, 8)

    def send(part, key, held, link):
        n = index[part][key]
        ref = arrays[part]
        slot = ref.at[wz(held[0]), wy(held[1]), c]
        i = names.index(part)
        which = 0 if n < 28 else 1
        return pltpu.make_async_remote_copy(
            src_ref=slot,
            dst_ref=slot,
            send_sem=send_sem.at[i, which],
            recv_sem=recv_sem.at[i, n],
            device_id=neighbour[link],
            device_id_type=MESH,
        )

    def wait_recv(part, key):
        n = index[part][key]
        i = names.index(part)
        slot = arrays[part].at[wz(key[0]), wy(key[1]), c]
        pltpu.make_async_remote_copy(
            src_ref=slot,
            dst_ref=slot,
            send_sem=send_sem.at[i, 0],
            recv_sem=recv_sem.at[i, n],
            device_id=sibling,
            device_id_type=MESH,
        ).wait_recv()

    def to_sibling(part, dz, cc):
        i = names.index(part)
        slots = arrays[part].at[wz(dz), :, cc]
        return pltpu.make_async_remote_copy(
            src_ref=slots,
            dst_ref=slots,
            send_sem=sib_send.at[i],
            recv_sem=sib_recv.at[i, DZS.index(dz)],
            device_id=sibling,
            device_id_type=MESH,
        )

    def one_to_sibling(part, dy, cc):
        i = names.index(part)
        slot = arrays[part].at[z, wy(dy), cc]
        return pltpu.make_async_remote_copy(
            src_ref=slot,
            dst_ref=slot,
            send_sem=sib_send.at[i],
            recv_sem=one_recv.at[i, DYS.index(dy)],
            device_id=sibling,
            device_id_type=MESH,
        )

    def together(ref, send=None, recv=None):
        copy = pltpu.make_async_remote_copy(
            src_ref=ref,
            dst_ref=ref,
            send_sem=drain_sem.at[0] if send is None else send,
            recv_sem=drain_sem.at[0] if recv is None else recv,
            device_id=sibling,
            device_id_type=MESH,
        )
        copy.wait_send() if send is not None else copy.wait_recv()

    def half(member):
        return ow.at[member, pl.ds(pl.multiple_of(128 * c, 128), 128)]

    def ow_copy(member, n, who):
        return pltpu.make_async_remote_copy(
            src_ref=half(member),
            dst_ref=half(member),
            send_sem=ow_send.at[0],
            recv_sem=ow_recv.at[0],
            device_id=who,
            device_id_type=MESH,
        )

    def other_half(member, mine):
        cc = c if mine else 1 - c
        return ow.at[member, pl.ds(pl.multiple_of(128 * cc, 128), 128)]

    def ow_sib(member, n, mine):
        ref = other_half(member, mine)
        return pltpu.make_async_remote_copy(
            src_ref=ref,
            dst_ref=ref,
            send_sem=ow_sib_send.at[0],
            recv_sem=ow_sib_recv.at[0],
            device_id=sibling,
            device_id_type=MESH,
        )

    def att_copy(member, n, who):
        return pltpu.make_async_remote_copy(
            src_ref=att.at[member],
            dst_ref=att.at[member],
            send_sem=att_send.at[0],
            recv_sem=att_recv.at[n],
            device_id=who,
            device_id_type=MESH,
        )

    def rs_copy(j, member, n, who):
        return pltpu.make_async_remote_copy(
            src_ref=part_buf.at[j, member],
            dst_ref=rs_buf.at[j, n],
            send_sem=rs_send.at[0],
            recv_sem=rs_recv.at[j],
            device_id=who,
            device_id_type=MESH,
        )

    def out_chunk(dz):
        return out_ref.at[x, :, pl.ds(pl.multiple_of(256 * wz(dz), 256), 256)]

    def ag_copy(j, who):
        return pltpu.make_async_remote_copy(
            src_ref=mine.at[j],
            dst_ref=out_chunk(DZS[j]),
            send_sem=ag_send.at[0],
            recv_sem=ag_recv.at[0],
            device_id=who,
            device_id_type=MESH,
        )

    def more():
        local[5].wait()
        ow_copy(x, 2, x_far).start()
        ow_copy(x, 0, x_plus).start()
        ow_copy(x, 1, x_minus).start()
        no = jnp.where(same, 0.0, 1.0).astype(BF16)
        no = jnp.concatenate([jnp.zeros((64, 256), BF16), no, jnp.zeros((48, 256), BF16)], axis=0)
        no_t = nt(eye(256), no)
        query_gain = jnp.concatenate([qg_ref[...], qg_ref[...]], axis=1)
        for pair in range(2):
            both = turned(q_ref[:, 128 * pair : 128 * pair + 128].astype(F32), query_gain) * 0.125
            for odd in range(2):
                head = pltpu.roll(both, 64, 1) if odd else both
                qs[2 * pair + odd] = jnp.where(low, head, no_t).astype(BF16)
        m_ref[...] = jnp.full((4, 256, 128), NEG, F32)
        l_ref[...] = jnp.zeros((4, 256, 128), F32)
        acc_ref[...] = jnp.zeros((4, 256, 64), F32)
        local[3].wait()
        local[4].wait()

    def ow_forward():
        together(ow.at[0:3, 0:128], recv=ow_recv.at[0])
        for n, member in enumerate((wx(-1), wx(1), wx(2))):
            ow_sib(member, n, True).start()

    def ow_wait():
        together(ow.at[0:3, 0:128], recv=ow_sib_recv.at[0])

    def attend(i):
        e0, e1, e2, e15 = (1 // (1 + (i - k) * (i - k)) for k in (0, 1, 2, 15))
        odd, start = lax.rem(i, 2), e0 + e1
        n = odd * ((i + 1) // 2) + (1 - odd) * (i // 2 - 1) + e0 - e1 + e2 - e15
        zz = lax.rem(z + NZ + (n + 1) // 2 * (2 * lax.rem(n, 2) - 1), NZ)
        cc = lax.rem(c + 1 - odd - e2 + e15, 2)
        pieces = [
            (
                start * lax.rem(y + 2 * i + j // 2, NY) + (1 - start) * j,
                start * (j % 2) + (1 - start) * cc,
            )
            for j in range(4)
        ]

        def scores(h):
            q = qs[h][:, :80]
            for j in range(4):
                s_ref[h % 2, :, 256 * j : 256 * j + 256] = nn(q, kt[zz, pieces[j][0], pieces[j][1]])

        scores(0)
        for h in range(4):
            if h < 3:
                scores(h + 1)
            for r in range(0, 256, 32):
                rows = slice(r, r + 32)
                sc = s_ref[h % 2, rows, :]
                old = m_ref[h, rows, :]
                new = jnp.maximum(old, jnp.max(sc, axis=1, keepdims=True))
                shrink = jnp.exp(old - new)
                m_ref[h, rows, :] = new
                w = jnp.exp(sc - new[:, :1])
                part = w[:, :128]
                for t in range(1, 8):
                    part = part + w[:, 128 * t : 128 * t + 128]
                l_ref[h, rows, :] = l_ref[h, rows, :] * shrink + part
                acc_ref[h, rows, :] = acc_ref[h, rows, :] * shrink[:, :64]
                p_ref[h % 2, rows, :] = w.astype(BF16)
            pv = nt(p_ref[h % 2, :, 0:256], vt[zz, pieces[0][0], pieces[0][1]])
            for j in range(1, 4):
                pv = pv + nt(p_ref[h % 2, :, 256 * j : 256 * j + 256], vt[zz, pieces[j][0], pieces[j][1]])
            acc_ref[h] = acc_ref[h] + pv

    def add(n, member, start):
        share = nn(att[member, 128 * n : 128 * n + 128, :], ow[member]).astype(BF16).astype(F32)
        if start is None:
            start = resid[2 * n : 2 * n + 2].reshape(128, 2048)
        resid[2 * n : 2 * n + 2] = (start + share).reshape(2, 64, 2048)

    def attended():
        pieces = []
        for h in range(4):
            total = jnp.sum(l_ref[h], axis=1, keepdims=True)
            pieces.append(acc_ref[h] / total)
        att[x] = jnp.concatenate(pieces, axis=1).astype(BF16)
        att_copy(x, 0, x_plus).start()
        att_copy(x, 1, x_minus).start()
        att_copy(x, 2, x_far).start()
        ow_wait()
        local[6].wait()
        for n in range(2):
            rows = slice(128 * n, 128 * n + 128)
            add(n, x, tok[rows, :].astype(F32))

    def mix(n):
        for half_rows in range(2):
            add(half_rows, wx((-1, 1, 2)[n]), None)

    def norm():
        for n in range(2):
            total = resid[2 * n : 2 * n + 2].reshape(128, 2048)
            mean = jnp.mean(total * total, axis=1, keepdims=True)
            scaled = (total * lax.rsqrt(mean + EPS) * ng_ref[...]).astype(BF16)
            for t in range(8):
                normed[t, 128 * n : 128 * n + 128, :] = scaled[:, 256 * t : 256 * t + 256]

    def gateup(n):
        cols = slice(256 * n, min(256 * n + 256, 1408))
        width = cols.stop - cols.start
        gate = jnp.zeros((256, width), F32)
        up = jnp.zeros((256, width), F32)
        for t in range(8):
            a = normed[t]
            gate = gate + nn(a, wg[t, :, :, :, cols].reshape(256, width))
            up = up + nn(a, wu[t, :, :, :, cols].reshape(256, width))
        hidden[:, cols] = (gate / (1.0 + jnp.exp(-gate)) * up).astype(BF16)

    def down(dz):
        j = DZS.index(dz)
        zz = wz(dz)
        fed = nt(hidden[:, :DOWN_A], wa[zz].reshape(256, DOWN_A))
        fed = (fed + nt(hidden[:, DOWN_A:], wb[zz].reshape(256, 1408 - DOWN_A))).astype(BF16)
        for member in range(4):
            part_buf[j, member] = fed[64 * member : 64 * member + 64]
        rs_copy(j, wx(2), 2, x_far).start()
        rs_copy(j, wx(1), 0, x_plus).start()
        rs_copy(j, wx(-1), 1, x_minus).start()

    def wait_rs(dz):
        j = DZS.index(dz)
        together(rs_buf.at[j], recv=rs_recv.at[j])

    def reduce(dz):
        j = DZS.index(dz)
        total = part_buf[j, x].astype(F32)
        for n in range(3):
            total = total + rs_buf[j, n].astype(F32)
        cols = pl.ds(pl.multiple_of(256 * wz(dz), 256), 256)
        mine[j] = (resid[x, :, cols] + total).astype(BF16)
        ag_copy(j, x_far).start()
        ag_copy(j, x_plus).start()
        ag_copy(j, x_minus).start()
        pltpu.make_async_copy(mine.at[j], out_chunk(dz), drain_sem.at[1]).start()

    def end():
        for i, name in enumerate(names):
            ref = arrays[name]
            many = ref.at[0:7, :, 0]
            few = ref.at[0, 0:3, 0]
            pltpu.make_async_remote_copy(
                src_ref=many,
                dst_ref=many,
                send_sem=send_sem.at[i, 0],
                recv_sem=recv_sem.at[i, 0],
                device_id=sibling,
                device_id_type=MESH,
            ).wait_send()
            pltpu.make_async_remote_copy(
                src_ref=few,
                dst_ref=few,
                send_sem=send_sem.at[i, 1],
                recv_sem=recv_sem.at[i, 0],
                device_id=sibling,
                device_id_type=MESH,
            ).wait_send()
            every = ref.at[:, :, c]
            pltpu.make_async_remote_copy(
                src_ref=every,
                dst_ref=every,
                send_sem=sib_send.at[i],
                recv_sem=recv_sem.at[i, 0],
                device_id=sibling,
                device_id_type=MESH,
            ).wait_send()
        together(ow.at[0:3, 0:128], send=ow_send.at[0])
        together(ow.at[0:3, 0:128], send=ow_sib_send.at[0])
        together(att.at[0:3], send=att_send.at[0])
        together(part_buf.at[0:6], send=rs_send.at[0])
        together(part_buf.at[0:6], send=ag_send.at[0])
        pltpu.make_async_copy(mine, mine, drain_sem.at[1]).wait()
        together(part_buf.at[0:6], recv=ag_recv.at[0])

    done = set()

    def handle(event):
        kind = event[0]
        if kind == "send":
            _, part, key, held, link = event
            if part in "gu" and part not in done:
                local[1 + "gu".index(part)].wait()
                done.add(part)
            send(part, key, held, link).start()
        elif kind == "wait":
            wait_recv(event[1], event[2])
        elif kind == "sib":
            to_sibling(event[1], event[2], c).start()
        elif kind == "one":
            one_to_sibling(event[1], event[2], c).start()
        elif kind == "waitone":
            one_to_sibling(event[1], event[2], 1 - c).wait_recv()
        elif kind == "waitsib":
            to_sibling(event[1], event[2], 1 - c).wait_recv()
        elif kind == "more":
            more()
        elif kind == "attended":
            attended()
        elif kind == "waitatt":
            att_copy(wx((-1, 1, 2)[event[1]]), event[1], x_far).wait_recv()
        elif kind == "mix":
            mix(event[1])
        elif kind == "norm":
            norm()
        elif kind == "gateup":
            gateup(event[1])
        elif kind == "down":
            down(event[1])
        elif kind == "waitrs":
            wait_rs(event[1])
        elif kind == "reduce":
            reduce(event[1])
        elif kind == "end":
            end()

    order, _ = plan()
    attends = [n for n, event in enumerate(order) if event[0] in ("first", "attend")]
    for event in order[: attends[0]]:
        handle(event)

    def step(i, carry):
        attend(i)
        for n in range(16):
            stop = attends[n + 1] if n < 15 else attends[15] + 1

            @pl.when(i == n)
            def _():
                for event in order[attends[n] + 1 : stop]:
                    handle(event)
                if n == 11:
                    ow_forward()

        return carry

    lax.fori_loop(0, 16, step, 0)
    for event in order[attends[15] + 1 :]:
        handle(event)


def per_device(
    tokens_in,
    queries,
    keys,
    values,
    doc_ids,
    query_gain,
    key_norm_scale,
    out_weight,
    norm_gain,
    gate_weight,
    up_weight,
    down_weight,
):
    row, col = turn_tables()
    vmem = pl.BlockSpec(memory_space=pltpu.VMEM)
    anywhere = pl.BlockSpec(memory_space=pl.ANY)
    hbm = pl.BlockSpec(memory_space=pltpu.HBM)
    dma = pltpu.SemaphoreType.DMA
    out = pl.pallas_call(
        kernel,
        name="layer",
        out_shape=jax.ShapeDtypeStruct((4, 64, 2048), BF16),
        in_specs=[hbm, vmem, vmem, hbm, vmem, vmem, vmem, hbm, vmem, hbm, hbm, hbm, vmem, vmem],
        out_specs=anywhere,
        scratch_shapes=[
            pltpu.VMEM((NZ, NY, NC, 80, 256), BF16),
            pltpu.VMEM((NZ, NY, NC, 64, 256), BF16),
            pltpu.VMEM((NZ, NY, NC, 32, 1408), BF16),
            pltpu.VMEM((NZ, NY, NC, 32, 1408), BF16),
            pltpu.VMEM((NZ, NY, NC, 32, DOWN_A), BF16),
            pltpu.VMEM((NZ, NY, NC, 32, 1408 - DOWN_A), BF16),
            pltpu.VMEM((4, 256, 2048), BF16),
            pltpu.VMEM((4, 256, 256), BF16),
            pltpu.VMEM((4, 256, 128), BF16),
            pltpu.VMEM((4, 256, 128), F32),
            pltpu.VMEM((4, 256, 128), F32),
            pltpu.VMEM((4, 256, 64), F32),
            pltpu.VMEM((2, 256, 1024), F32),
            pltpu.VMEM((2, 256, 1024), BF16),
            pltpu.VMEM((256, 2048), BF16),
            pltpu.VMEM((4, 64, 2048), F32),
            pltpu.VMEM((8, 256, 256), BF16),
            pltpu.VMEM((256, 1408), BF16),
            pltpu.VMEM((8, 4, 64, 256), BF16),
            pltpu.VMEM((8, 3, 64, 256), BF16),
            pltpu.VMEM((8, 64, 256), BF16),
            dma((6, 31)),
            dma((6, 2)),
            dma((6, 8)),
            dma((6,)),
            dma((1,)),
            dma((1,)),
            dma((1,)),
            dma((1,)),
            dma((3,)),
            dma((1,)),
            dma((8,)),
            dma((1,)),
            dma((1,)),
            dma((1,)),
            dma((7,)),
            dma((2,)),
            dma((2, 4)),
        ],
        compiler_params=pltpu.CompilerParams(
            collective_id=0, has_side_effects=True, vmem_limit_bytes=60 * 1024 * 1024
        ),
    )(
        tokens_in,
        queries,
        keys.T,
        values.T,
        doc_ids.reshape(1, -1),
        query_gain.reshape(1, -1),
        key_norm_scale.reshape(1, -1),
        out_weight,
        norm_gain.reshape(1, -1),
        gate_weight,
        up_weight,
        down_weight.T,
        jnp.asarray(row),
        jnp.asarray(col),
    )
    return out.reshape(256, 2048)


def solution(mesh):
    return jax.shard_map(
        per_device,
        mesh=mesh,
        in_specs=(
            P("sp", None),
            P("sp", "tp"),
            P("sp", "tp"),
            P("sp", "tp"),
            P("sp"),
            P(),
            P(),
            P("tp", None),
            P(),
            P("sp", "tp"),
            P("sp", "tp"),
            P("tp", "sp"),
        ),
        out_specs=P("sp", None),
        check_vma=False,
    )
```
